256 devices in a mesh: fs: 32 (over z, x), tp: 8 (over y, core).
Axes of the slice: x: 4, y: 4, z: 8, core: 2. Of those that a mesh axis runs over, the one named last changes fastest.
Arguments:
- tokens: bfloat16 [8192, 1536], P('fs', 'tp'), may hold values from -6 to 6
- norm_in_gain: float32 [1536], replicated, may hold values from 0.1 to 1.9
- query_w: bfloat16 [1536, 768], P('fs', 'tp'), may hold values from -0.15625 to 0.15625
- key_w: bfloat16 [1536, 768], P('fs', 'tp'), may hold values from -0.15625 to 0.15625
- value_w: bfloat16 [1536, 768], P('fs', 'tp'), may hold values from -0.15625 to 0.15625
- gate_w: bfloat16 [1536, 768], P('fs', 'tp'), may hold values from -0.15625 to 0.15625
- out_w: bfloat16 [768, 1536], P('tp', 'fs'), may hold values from -0.21875 to 0.21875
- norm_mid_gain: float32 [1536], replicated, may hold values from 0.1 to 1.9
- up_gate_w: bfloat16 [1536, 4096], P('fs', 'tp'), may hold values from -0.15625 to 0.15625
- up_value_w: bfloat16 [1536, 4096], P('fs', 'tp'), may hold values from -0.15625 to 0.15625
- conv_taps: float32 [3, 4096], P(None, 'tp'), may hold values from -3.5 to 3.5
- conv_bias: float32 [4096], P('tp'), may hold values from -3 to 3
- down_w: bfloat16 [4096, 1536], P('tp', 'fs'), may hold values from -0.09375 to 0.09375
Outputs:
- layer_out: bfloat16 [8192, 1536], P('fs', 'tp')
The draws below stay inside these ranges and needn't reach their ends.
All inputs are finite; a program needn't handle non-finite values.
Results may differ from the reference program's by a relative error of at most 0.02.
Values may be sent and summed in bfloat16 or wider, within the bound.
No kernel may reach another device: no remote copies, remote signals or barrier semaphores. Data moves between devices by JAX's collectives and lax.ppermute only.
A program may use at most 64 MiB of HBM per device.

```python
import jax
import jax.numpy as jnp
from jax import lax

D = 1536
FF = 4096
HEADS = 8
BLOCK = 32
CONV = 3
TOK = 256
HEAD_DIM = 96
TOKENS = 8192
N_FS = 32


def shard_levels(stream_key, dims, split, low, high):
    gain = 1.0
    for dim, shards_of in split:
        draws = jax.random.uniform(jax.random.fold_in(jax.random.fold_in(stream_key, 6), dim), (shards_of,), jnp.float32, low / len(split), high / len(split))
        gain = gain * jnp.repeat(jnp.exp(draws), dims[dim] // shards_of).reshape((-1,) + (1,) * (len(dims) - 1 - dim))
    return gain


def normal_values(own_key, extent, spread, bound, cuts=(), kind=jnp.bfloat16):
    entries = spread * jax.random.normal(own_key, extent, jnp.float32)
    if cuts:
        entries = entries * shard_levels(own_key, extent, cuts, -0.22, 0.18)
    return jnp.clip(entries, -bound, bound).astype(kind)


def setup_inputs(seed: int = 0) -> dict:
    keys = jax.random.split(jax.random.key(seed), 14)
    return {
        "tokens": normal_values(keys[0], (TOKENS, D), 1.0, 6.0, ((0, 32), (1, 8))),
        "norm_in_gain": jnp.clip(1.0 + 0.18 * jax.random.normal(keys[1], (D,), jnp.float32), 0.1, 1.9),
        "query_w": normal_values(keys[2], (D, D // 2), D ** -0.5, 0.15625, ((0, 32), (1, 8))),
        "key_w": normal_values(keys[3], (D, D // 2), D ** -0.5, 0.15625, ((0, 32), (1, 8))),
        "value_w": normal_values(keys[4], (D, D // 2), D ** -0.5, 0.15625, ((0, 32), (1, 8))),
        "gate_w": normal_values(keys[5], (D, D // 2), D ** -0.5, 0.15625, ((0, 32), (1, 8))),
        "out_w": normal_values(keys[6], (D // 2, D), (D // 2) ** -0.5, 0.21875, ((0, 8), (1, 32))),
        "norm_mid_gain": jnp.clip(1.0 + 0.18 * jax.random.normal(keys[7], (D,), jnp.float32), 0.1, 1.9),
        "up_gate_w": normal_values(keys[8], (D, FF), D ** -0.5, 0.15625, ((0, 32), (1, 8))),
        "up_value_w": normal_values(keys[9], (D, FF), D ** -0.5, 0.15625, ((0, 32), (1, 8))),
        "conv_taps": normal_values(keys[10], (CONV, FF), CONV ** -0.5, 3.5, ((1, 8),), jnp.float32),
        "conv_bias": normal_values(keys[11], (FF,), 0.5, 3.0, ((0, 8),), jnp.float32),
        "down_w": normal_values(keys[12], (FF, D), FF ** -0.5, 0.09375, ((0, 8), (1, 32))),
    }


epsilon = 1e-06
rotary_base = 10000.0

def rms_scale(row_block, gain_row):
    widened = row_block.astype(jnp.float32)
    scaled = widened * lax.rsqrt(lax.optimization_barrier(jnp.mean(widened * widened, axis=-1, keepdims=True)) + epsilon)
    return (scaled * gain_row).astype(jnp.bfloat16)

def rotate(values_in, positions):
    half_width = values_in.shape[-1] // 2
    inv_freq = jnp.power(rotary_base, -jnp.arange(half_width, dtype=jnp.float32) / half_width)
    angles = positions[:, None] * inv_freq[None, :]
    cosine = jnp.cos(angles)[:, None, :]
    sine = jnp.sin(angles)[:, None, :]
    widened = values_in.astype(jnp.float32)
    first_half = widened[..., :half_width]
    second_half = widened[..., half_width:]
    return jnp.concatenate([first_half * cosine - second_half * sine, first_half * sine + second_half * cosine], axis=-1)

def retain(query_h, key_h, value_h, log_gamma, block_size):
    length, head_count, head_width = query_h.shape
    blocks = length // block_size
    offsets = jnp.arange(block_size, dtype=jnp.float32)
    lag_grid = offsets[:, None] - offsets[None, :]
    intra_decay = jnp.where(lag_grid[None] >= 0, jnp.exp(log_gamma[:, None, None] * jnp.maximum(lag_grid, 0.0)[None]), 0.0)
    query_decay = jnp.exp(log_gamma[None, :] * (offsets + 1.0)[:, None])
    key_decay = jnp.exp(log_gamma[None, :] * (block_size - 1.0 - offsets)[:, None])
    block_decay = jnp.exp(log_gamma * block_size)
    query_b = query_h.astype(jnp.float32).reshape(blocks, block_size, head_count, head_width)
    key_b = key_h.astype(jnp.float32).reshape(blocks, block_size, head_count, head_width)
    value_b = value_h.astype(jnp.float32).reshape(blocks, block_size, head_count, head_width)
    scores = jnp.einsum('nchd,nshd->nhcs', query_b, key_b, precision=lax.Precision.HIGHEST) * intra_decay[None]
    within = jnp.einsum('nhcs,nshe->nche', scores, value_b, precision=lax.Precision.HIGHEST)

    def advance(memory, block_inputs):
        query_n, key_n, value_n = block_inputs
        across_n = jnp.einsum('chd,hde->che', query_n * query_decay[:, :, None], memory, precision=lax.Precision.HIGHEST)
        memory = memory * block_decay[:, None, None] + jnp.einsum('chd,che->hde', key_n * key_decay[:, :, None], value_n, precision=lax.Precision.HIGHEST)
        return (memory, across_n)
    initial = jnp.zeros((head_count, head_width, head_width), jnp.float32)
    final_memory, across = lax.scan(advance, initial, (query_b, key_b, value_b))
    return (within + across).reshape(length, head_count, head_width)

def mix_heads(queries, key_m, value_m, gate_m, log_gamma, head_width, block_size):
    length = queries.shape[0]
    head_count = queries.shape[1] // head_width
    positions = jnp.arange(length, dtype=jnp.float32)
    query_r = rotate(queries.reshape(length, head_count, head_width), positions).astype(jnp.bfloat16)
    key_r = (rotate(key_m.reshape(length, head_count, head_width), positions) * head_width ** (-0.5)).astype(jnp.bfloat16)
    retained = retain(query_r, key_r, value_m.reshape(length, head_count, head_width), log_gamma, block_size)
    normed = retained * lax.rsqrt(lax.optimization_barrier(jnp.mean(retained * retained, axis=-1, keepdims=True)) + epsilon)
    return (normed.reshape(length, -1) * jax.nn.silu(gate_m.astype(jnp.float32))).astype(jnp.bfloat16)

def convolve(gate_up, conv_taps, conv_bias):
    length = gate_up.shape[0]
    tap_count = conv_taps.shape[0]
    padded = jnp.pad(gate_up.astype(jnp.float32), ((tap_count - 1, 0), (0, 0)))
    summed = jnp.zeros(gate_up.shape, jnp.float32) + conv_bias[None, :]
    for tap_index in range(tap_count):
        summed = summed + padded[tap_index:tap_index + length] * conv_taps[tap_index][None, :]
    return summed

def reference(tokens, norm_in_gain, query_w, key_w, value_w, gate_w, out_w, norm_mid_gain, up_gate_w, up_value_w, conv_taps, conv_bias, down_w):
    normed_in = rms_scale(tokens, norm_in_gain)

    def project(normed, weight):
        return jnp.dot(normed, weight, preferred_element_type=jnp.float32).astype(jnp.bfloat16)

    def by_sequence(matrix):
        return matrix.reshape(N_FS, TOK, matrix.shape[-1])
    queries = project(normed_in, query_w)
    key_m = project(normed_in, key_w)
    value_m = project(normed_in, value_w)
    gate_m = project(normed_in, gate_w)
    log_gamma = jnp.log1p(-jnp.exp2(-5.0 - jnp.arange(HEADS, dtype=jnp.float32)))
    gated_heads = jax.vmap(lambda q_part, k_part, v_part, g_part: mix_heads(q_part, k_part, v_part, g_part, log_gamma, HEAD_DIM, BLOCK))(by_sequence(queries), by_sequence(key_m), by_sequence(value_m), by_sequence(gate_m)).reshape(N_FS * TOK, -1)
    mixer_out = jnp.dot(gated_heads, out_w, preferred_element_type=jnp.float32)
    middle = (tokens.astype(jnp.float32) + mixer_out).astype(jnp.bfloat16)
    normed_mid = rms_scale(middle, norm_mid_gain)
    gate_up = project(normed_mid, up_gate_w)
    value_up = project(normed_mid, up_value_w)
    convolved = jax.vmap(lambda g_part: convolve(g_part, conv_taps, conv_bias))(by_sequence(gate_up)).reshape(N_FS * TOK, -1)
    hidden = (jax.nn.silu(convolved) * value_up.astype(jnp.float32)).astype(jnp.bfloat16)
    return (middle.astype(jnp.float32) + jnp.dot(hidden, down_w, preferred_element_type=jnp.float32)).astype(jnp.bfloat16)
```

```python
import functools

import jax
import jax.numpy as jnp
import numpy as np
from jax import lax
from jax.experimental import pallas as pl
from jax.experimental.pallas import tpu as pltpu
from jax.sharding import Mesh
from jax.sharding import PartitionSpec as P

HEAD_DIM = 96
HALF = HEAD_DIM // 2
NZ, NX, NY, NC = 8, 4, 4, 2
FS = ("z", "x")
TP = ("y", "c")
EPS = 1e-06
BASE = 10000.0
F32, BF16 = jnp.float32, jnp.bfloat16


def shift(axis, n, k):
    pairs = [(i, (i + k) % n) for i in range(n)]
    return lambda a: lax.ppermute(a, axis, pairs)


def Z(k):
    return shift("z", NZ, k)


def X(k):
    return shift("x", NX, k)


def Y(k):
    return shift("y", NY, k)


swap = shift("c", NC, 1)


def ring_z(own, cut):
    f1, b1, f2, b2 = Z(1)(own), Z(-1)(own), Z(2)(own), Z(-2)(own)
    lo, _ = cut(f2)
    _, hi = cut(b2)
    f3, b3, f4, b4 = Z(1)(f2), Z(-1)(b2), Z(2)(lo), Z(-2)(hi)
    return own, b1, b2, b3, (f4, b4), f3, f2, f1


def of_tp(own):
    same = jnp.stack([own, Y(-1)(own), Y(2)(own), Y(1)(own)])
    return same, swap(same)


def to_tp(keep, send):
    both = keep.astype(F32) + swap(send).astype(F32)
    out = both.astype(BF16)
    got = (Y(1)(out[1]), Y(2)(out[2]), Y(-1)(out[3]))
    return both[0] + sum(g.astype(F32) for g in got)


def dot(a, b, ca, cb):
    return lax.dot_general(a, b, (((ca,), (cb,)), ((), ())), preferred_element_type=F32)


def normalize(ids, same, other, gain, xn):
    y, c = ids[2], ids[3]
    total = jnp.zeros((1, xn.shape[-1]), F32)
    for k in range(NY):
        for ref in (same, other):
            v = ref[k].astype(F32)
            total = total + jnp.sum(v * v, axis=0, keepdims=True)
    count = NZ * NX * xn.shape[2]
    scale = lax.rsqrt(total / count + EPS)
    for k in range(NY):
        for ref, core in ((same, c), (other, 1 - c)):
            t = lax.rem(y + k, NY) * NC + core
            v = ref[k].astype(F32) * scale
            v = v * gain[t]
            xn[t] = v.astype(BF16).reshape(xn.shape[1:])


def give(ids, m, block, keep, send):
    z, x, y, c = ids[0], ids[1], ids[2], ids[3]
    t = lax.rem(z + m, NZ)
    k = lax.rem(t // NC + NY - y, NY)
    mine = lax.rem(t, NC) == c
    block = block.astype(BF16).reshape(NX, -1, block.shape[-1])

    @pl.when(mine)
    def _():
        for j in range(NX):
            keep[k, lax.rem(x + j, NX)] = block[j]

    @pl.when(jnp.logical_not(mine))
    def _():
        for j in range(NX):
            send[k, lax.rem(x + j, NX)] = block[j]


def mixer_kernel(ids, same, other, gain, decay, cos, sin, turn, *refs):
    pieces, (keep, send, xn, xr, wr) = refs[:9], refs[9:]
    z, x = ids[0], ids[1]
    normalize(ids, same, other, gain, xn)
    rows = xn.shape[2]
    span = NX * rows
    for m in range(NZ):
        for j in range(NX):
            at = (m * NX + j) * rows
            xr[at : at + rows, :] = xn[lax.rem(z + m, NZ), lax.rem(x + j, NX)]
    place = 0
    for ref in pieces:
        wr[place : place + ref.shape[0], :] = ref[...]
        place += ref.shape[0]
    out = dot(xr[...], wr[:, : 4 * HEAD_DIM], 0, 0).astype(BF16)
    q, k, v, g = (out[:, i * HEAD_DIM : (i + 1) * HEAD_DIM] for i in range(4))
    flip = turn[...]
    qr = (q.astype(F32) * cos[...] + dot(q, flip, 1, 0) * sin[...]).astype(BF16)
    kr = (k.astype(F32) * cos[...] + dot(k, flip, 1, 0) * sin[...]) * HEAD_DIM ** (-0.5)
    kr = kr.astype(BF16)
    scores = dot(qr, kr, 1, 1) * decay[...]
    kept = dot(scores.astype(BF16), v, 1, 0)
    normed = kept * lax.rsqrt(jnp.mean(kept * kept, axis=-1, keepdims=True) + EPS)
    gate = g.astype(F32)
    gated = (normed * (gate * jax.nn.sigmoid(gate))).astype(BF16)
    for m in range(NZ):
        block = dot(wr[m * span : (m + 1) * span, 4 * HEAD_DIM :], gated, 1, 1)
        give(ids, m, block, keep, send)


def channel_kernel(ids, same, other, gain, taps, bias, *refs):
    ups, downs, (keep, send, xn, xr) = refs[:4], refs[4:13], refs[13:]
    z, x = ids[0], ids[1]
    normalize(ids, same, other, gain, xn)
    rows = xn.shape[2]
    acc = None
    for j in range(NX):
        for m in range(NZ):
            xr[m * rows : (m + 1) * rows, :] = xn[lax.rem(z + m, NZ), lax.rem(x + j, NX)]
        part = dot(xr[...], ups[j][...], 0, 0)
        acc = part if acc is None else acc + part
    width = acc.shape[1] // 2
    gate = acc[:, :width].astype(BF16).astype(F32)
    value = acc[:, width:].astype(BF16).astype(F32)
    taps_n = taps.shape[0]
    row = lax.broadcasted_iota(jnp.int32, gate.shape, 0)
    total = jnp.zeros_like(gate) + bias[...]
    for i in range(taps_n):
        back = taps_n - 1 - i
        moved = gate if back == 0 else jnp.where(row >= back, pltpu.roll(gate, back, 0), 0.0)
        total = total + moved * taps[i : i + 1, :]
    hidden = (total * jax.nn.sigmoid(total) * value).astype(BF16)
    halves = [r[...] for r in downs]
    blocks = halves[:4] + [jnp.concatenate(halves[4:6], axis=0)] + halves[6:]
    for m in range(NZ):
        give(ids, m, dot(blocks[m], hidden, 1, 1), keep, send)


def call(kernel, ids, args, length, rows, scratch, flops, moved):
    out = jax.ShapeDtypeStruct((NY, NX, rows, length), BF16)
    vmem = pl.BlockSpec(memory_space=pltpu.VMEM)
    keep, send = pl.pallas_call(
        kernel,
        out_shape=(out, out),
        in_specs=[pl.BlockSpec(memory_space=pltpu.SMEM)] + [vmem] * len(args),
        out_specs=(vmem, vmem),
        scratch_shapes=scratch,
        compiler_params=pltpu.CompilerParams(vmem_limit_bytes=48 * 1024 * 1024),
        cost_estimate=pl.CostEstimate(flops=flops, bytes_accessed=moved, transcendentals=0),
    )(ids, *args)
    span = NX * rows
    return keep.reshape(NY, span, length), send.reshape(NY, span, length)


def tables(length):
    inv = np.power(np.float32(BASE), -np.arange(HALF, dtype=np.float32) / np.float32(HALF))
    angles = np.arange(length, dtype=np.float32)[:, None] * inv.astype(np.float32)[None, :]
    cos, sin = np.cos(angles).astype(np.float32), np.sin(angles).astype(np.float32)
    turn = np.zeros((HEAD_DIM, HEAD_DIM), np.float32)
    for i in range(HALF):
        turn[i + HALF, i] = -1.0
        turn[i, i + HALF] = 1.0
    return np.concatenate([cos, cos], 1), np.concatenate([sin, sin], 1), turn


def per_device(
    tokens,
    norm_in_gain,
    query_w,
    key_w,
    value_w,
    gate_w,
    out_w,
    norm_mid_gain,
    up_gate_w,
    up_value_w,
    conv_taps,
    conv_bias,
    down_w,
):
    length = tokens.shape[0]
    rows = query_w.shape[0]
    span = NX * rows
    width = conv_bias.shape[0]
    z, x, y, c = (lax.axis_index(a) for a in ("z", "x", "y", "c"))
    ids = jnp.stack([z, x, y, c]).astype(jnp.int32)
    own = tokens.T

    attn = jnp.concatenate([query_w, key_w, value_w, gate_w, out_w.T], axis=1)
    first = jnp.concatenate([attn, down_w.T], axis=1)
    quads = jnp.concatenate([first, X(-1)(first), X(2)(first), X(1)(first)], axis=0)
    cut = attn.shape[1]
    half = span // 2
    mixer_w = ring_z(quads[:, :cut], lambda a: (a[:half], a[half:]))
    up = jnp.concatenate([up_gate_w, up_value_w], axis=1)
    ups = ring_z(up, lambda a: (a[:, :width], a[:, width:]))
    ups = jnp.concatenate(
        list(ups[:4]) + [jnp.concatenate(ups[4], axis=1)] + list(ups[5:]), axis=0
    )
    ups = (ups, X(-1)(ups), X(2)(ups), X(1)(ups))
    downs = ring_z(quads[:, cut:], lambda a: (a[:half], a[half:]))

    def flat(blocks):
        return list(blocks[:4]) + list(blocks[4]) + list(blocks[5:])

    head = (y * NC + c).astype(F32)
    log_gamma = jnp.log1p(-jnp.exp2(-5.0 - head))
    lag = jnp.arange(length, dtype=F32)[:, None] - jnp.arange(length, dtype=F32)[None, :]
    decay = jnp.where(lag >= 0, jnp.exp(log_gamma * jnp.maximum(lag, 0.0)), 0.0)
    cos, sin, turn = tables(length)

    features = NZ * span
    canon = (NZ, NX, rows, length)
    same, other = of_tp(own)
    keep, send = call(
        mixer_kernel,
        ids,
        [same, other, norm_in_gain.reshape(NZ, span, 1), decay, jnp.asarray(cos), jnp.asarray(sin)]
        + [jnp.asarray(turn, BF16)]
        + flat(mixer_w),
        length,
        rows,
        [
            pltpu.VMEM(canon, BF16),
            pltpu.VMEM((features, length), BF16),
            pltpu.VMEM((features, cut), BF16),
        ],
        2 * length * features * cut * 2,
        8 * features * length,
    )
    middle = (own.astype(F32) + to_tp(keep, send)).astype(BF16)
    same, other = of_tp(middle)
    keep, send = call(
        channel_kernel,
        ids,
        [same, other, norm_mid_gain.reshape(NZ, span, 1), conv_taps, conv_bias.reshape(1, width)]
        + list(ups)
        + flat(downs),
        length,
        rows,
        [pltpu.VMEM(canon, BF16), pltpu.VMEM((NZ * rows, length), BF16)],
        2 * length * features * width * 3,
        8 * features * length,
    )
    return (middle.astype(F32) + to_tp(keep, send)).astype(BF16).T


def solution(mesh):
    finer = Mesh(mesh.devices.reshape(NZ, NX, NY, NC), ("z", "x", "y", "c"))
    return jax.shard_map(
        per_device,
        mesh=finer,
        in_specs=(
            P(FS, TP),
            P(),
            P(FS, TP),
            P(FS, TP),
            P(FS, TP),
            P(FS, TP),
            P(TP, FS),
            P(),
            P(FS, TP),
            P(FS, TP),
            P(None, TP),
            P(TP),
            P(TP, FS),
        ),
        out_specs=P(FS, TP),
        check_vma=False,
    )
```

```python
import functools

import jax
import jax.numpy as jnp
import numpy as np
from jax import lax
from jax.experimental import pallas as pl
from jax.experimental.pallas import tpu as pltpu
from jax.sharding import Mesh
from jax.sharding import PartitionSpec as P

HEAD_DIM = 96
HALF = HEAD_DIM // 2
NZ, NX, NY, NC = 8, 4, 4, 2
FS = ("z", "x")
TP = ("y", "c")
EPS = 1e-06
BASE = 10000.0
F32, BF16 = jnp.float32, jnp.bfloat16


def shift(axis, n, k):
    pairs = [(i, (i + k) % n) for i in range(n)]
    return lambda a: lax.ppermute(a, axis, pairs)


def Z(k):
    return shift("z", NZ, k)


def X(k):
    return shift("x", NX, k)


def Y(k):
    return shift("y", NY, k)


swap = shift("c", NC, 1)


def ring_z(own):
    half = own.shape[0] // 2
    f, b = [own], [own]
    for _ in range(3):
        f.append(Z(1)(f[-1]))
        b.append(Z(-1)(b[-1]))
    last = (Z(1)(f[3][:half]), Z(-1)(b[3][half:]))
    return [own, b[1], b[2], b[3], last[0], last[1], f[3], f[2], f[1]]


def spread(own, axis, n):
    return lax.all_to_all(jnp.broadcast_to(own[None], (n,) + own.shape), axis, 0, 0)


def of_tp(own):
    same = jnp.stack([own, Y(-1)(own), Y(2)(own), Y(1)(own)])
    return same, swap(same)


def to_tp(keep, send):
    both = keep.astype(F32) + swap(send).astype(F32)
    out = both.astype(BF16)
    got = (Y(1)(out[1]), Y(2)(out[2]), Y(-1)(out[3]))
    return both[0] + sum(g.astype(F32) for g in got)


def dot(a, b, ca, cb):
    return lax.dot_general(a, b, (((ca,), (cb,)), ((), ())), preferred_element_type=F32)


def normalize(ids, same, other, gain, xn):
    y, c = ids[2], ids[3]

    def square(k, total):
        for ref in (same, other):
            v = ref[k].astype(F32)
            total = total + jnp.sum(v * v, axis=0, keepdims=True)
        return total

    total = lax.fori_loop(0, NY, square, jnp.zeros((1, xn.shape[-1]), F32))
    count = NZ * NX * xn.shape[2]
    scale = lax.rsqrt(total / count + EPS)

    def fill(k, _):
        for ref, core in ((same, c), (other, 1 - c)):
            t = lax.rem(y + k, NY) * NC + core
            v = ref[k].astype(F32) * scale
            v = v * gain[t]
            xn[t] = v.astype(BF16).reshape(xn.shape[1:])
        return 0

    lax.fori_loop(0, NY, fill, 0)


def give(ids, m, block, keep, send):
    z, x, y, c = ids[0], ids[1], ids[2], ids[3]
    t = lax.rem(z + m, NZ)
    k = lax.rem(t // NC + NY - y, NY)
    mine = lax.rem(t, NC) == c
    block = block.astype(BF16).reshape(NX, -1, block.shape[-1])

    @pl.when(mine)
    def _():
        for j in range(NX):
            keep[k, lax.rem(x + j, NX)] = block[j]

    @pl.when(jnp.logical_not(mine))
    def _():
        for j in range(NX):
            send[k, lax.rem(x + j, NX)] = block[j]


def mixer_kernel(ids, same, other, gain, decay, cos, sin, turn, *refs):
    pieces, (keep, send, xn, xr, wr) = refs[:9], refs[9:]
    z, x = ids[0], ids[1]
    normalize(ids, same, other, gain, xn)
    rows = xn.shape[2]
    span = NX * rows

    def pick(m, _):
        for j in range(NX):
            xr[pl.ds(pl.multiple_of((m * NX + j) * rows, rows), rows), :] = xn[
                lax.rem(z + m, NZ), lax.rem(x + j, NX)
            ]
        return 0

    lax.fori_loop(0, NZ, pick, 0)
    place = 0
    for ref in pieces:
        wr[place : place + ref.shape[0], :] = ref[...]
        place += ref.shape[0]
    out = dot(xr[...], wr[:, : 4 * HEAD_DIM], 0, 0).astype(BF16)
    q, k, v, g = (out[:, i * HEAD_DIM : (i + 1) * HEAD_DIM] for i in range(4))
    flip = turn[...]
    qr = (q.astype(F32) * cos[...] + dot(q, flip, 1, 0) * sin[...]).astype(BF16)
    kr = (k.astype(F32) * cos[...] + dot(k, flip, 1, 0) * sin[...]) * HEAD_DIM ** (-0.5)
    kr = kr.astype(BF16)
    scores = dot(qr, kr, 1, 1) * decay[...]
    kept = dot(scores.astype(BF16), v, 1, 0)
    normed = kept * lax.rsqrt(jnp.mean(kept * kept, axis=-1, keepdims=True) + EPS)
    gate = g.astype(F32)
    gated = (normed * (gate * jax.nn.sigmoid(gate))).astype(BF16)

    def project(m, _):
        rows_m = wr[pl.ds(pl.multiple_of(m * span, span), span), 4 * HEAD_DIM :]
        give(ids, m, dot(rows_m, gated, 1, 1), keep, send)
        return 0

    lax.fori_loop(0, NZ, project, 0)


def channel_kernel(ids, same, other, gain, taps, bias, *refs):
    ups, downs, (keep, send, xn, xr, acc) = refs[:4], refs[4], refs[5:]
    x = ids[1]
    normalize(ids, same, other, gain, xn)
    rows = xn.shape[2]
    for j in range(NX):

        def pick(m, _):
            xr[pl.ds(pl.multiple_of(m * rows, rows), rows), :] = xn[m, lax.rem(x + j, NX)]
            return 0

        lax.fori_loop(0, NZ, pick, 0)
        part = dot(xr[...], ups[j][...], 0, 0)
        acc[...] = part if j == 0 else acc[...] + part
    width = acc.shape[1] // 2
    gate = acc[:, :width].astype(BF16).astype(F32)
    value = acc[:, width:].astype(BF16).astype(F32)
    taps_n = taps.shape[0]
    row = lax.broadcasted_iota(jnp.int32, gate.shape, 0)
    total = jnp.zeros_like(gate) + bias[...]
    for i in range(taps_n):
        back = taps_n - 1 - i
        moved = gate if back == 0 else jnp.where(row >= back, pltpu.roll(gate, back, 0), 0.0)
        total = total + moved * taps[i : i + 1, :]
    hidden = (total * jax.nn.sigmoid(total) * value).astype(BF16)

    def project(t, _):
        give(ids, lax.rem(t + NZ - ids[0], NZ), dot(downs[t], hidden, 1, 1), keep, send)
        return 0

    lax.fori_loop(0, NZ, project, 0)


def call(kernel, ids, args, length, rows, scratch, flops, moved):
    out = jax.ShapeDtypeStruct((NY, NX, rows, length), BF16)
    vmem = pl.BlockSpec(memory_space=pltpu.VMEM)
    keep, send = pl.pallas_call(
        kernel,
        out_shape=(out, out),
        in_specs=[pl.BlockSpec(memory_space=pltpu.SMEM)] + [vmem] * len(args),
        out_specs=(vmem, vmem),
        scratch_shapes=scratch,
        compiler_params=pltpu.CompilerParams(vmem_limit_bytes=48 * 1024 * 1024),
        cost_estimate=pl.CostEstimate(flops=flops, bytes_accessed=moved, transcendentals=0),
    )(ids, *args)
    span = NX * rows
    return keep.reshape(NY, span, length), send.reshape(NY, span, length)


def tables(length):
    inv = np.power(np.float32(BASE), -np.arange(HALF, dtype=np.float32) / np.float32(HALF))
    angles = np.arange(length, dtype=np.float32)[:, None] * inv.astype(np.float32)[None, :]
    cos, sin = np.cos(angles).astype(np.float32), np.sin(angles).astype(np.float32)
    turn = np.zeros((HEAD_DIM, HEAD_DIM), np.float32)
    for i in range(HALF):
        turn[i + HALF, i] = -1.0
        turn[i, i + HALF] = 1.0
    return np.concatenate([cos, cos], 1), np.concatenate([sin, sin], 1), turn


def per_device(
    tokens,
    norm_in_gain,
    query_w,
    key_w,
    value_w,
    gate_w,
    out_w,
    norm_mid_gain,
    up_gate_w,
    up_value_w,
    conv_taps,
    conv_bias,
    down_w,
):
    length = tokens.shape[0]
    rows = query_w.shape[0]
    span = NX * rows
    width = conv_bias.shape[0]
    z, x, y, c = (lax.axis_index(a) for a in ("z", "x", "y", "c"))
    ids = jnp.stack([z, x, y, c]).astype(jnp.int32)
    own = tokens.T

    attn = jnp.concatenate([query_w, key_w, value_w, gate_w, out_w.T], axis=1)
    first = jnp.concatenate([attn, down_w.T], axis=1)
    quads = jnp.concatenate([first, X(-1)(first), X(2)(first), X(1)(first)], axis=0)
    cut = attn.shape[1]
    mixer_w = ring_z(quads[:, :cut])
    up = jnp.concatenate([up_gate_w, up_value_w], axis=1)
    ups = spread(up, "z", NZ).reshape(NZ * rows, 2 * width)
    ups = (ups, X(-1)(ups), X(2)(ups), X(1)(ups))
    downs = spread(quads[:, cut:], "z", NZ)

    head = (y * NC + c).astype(F32)
    log_gamma = jnp.log1p(-jnp.exp2(-5.0 - head))
    lag = jnp.arange(length, dtype=F32)[:, None] - jnp.arange(length, dtype=F32)[None, :]
    decay = jnp.where(lag >= 0, jnp.exp(log_gamma * jnp.maximum(lag, 0.0)), 0.0)
    cos, sin, turn = tables(length)

    features = NZ * span
    canon = (NZ, NX, rows, length)
    same, other = of_tp(own)
    keep, send = call(
        mixer_kernel,
        ids,
        [same, other, norm_in_gain.reshape(NZ, span, 1), decay, jnp.asarray(cos), jnp.asarray(sin)]
        + [jnp.asarray(turn, BF16)]
        + mixer_w,
        length,
        rows,
        [
            pltpu.VMEM(canon, BF16),
            pltpu.VMEM((features, length), BF16),
            pltpu.VMEM((features, cut), BF16),
        ],
        2 * length * features * cut * 2,
        8 * features * length,
    )
    middle = (own.astype(F32) + to_tp(keep, send)).astype(BF16)
    same, other = of_tp(middle)
    keep, send = call(
        channel_kernel,
        ids,
        [same, other, norm_mid_gain.reshape(NZ, span, 1), conv_taps, conv_bias.reshape(1, width)]
        + list(ups)
        + [downs],
        length,
        rows,
        [
            pltpu.VMEM(canon, BF16),
            pltpu.VMEM((NZ * rows, length), BF16),
            pltpu.VMEM((length, 2 * width), F32),
        ],
        2 * length * features * width * 3,
        8 * features * length,
    )
    return (middle.astype(F32) + to_tp(keep, send)).astype(BF16).T


def solution(mesh):
    finer = Mesh(mesh.devices.reshape(NZ, NX, NY, NC), ("z", "x", "y", "c"))
    return jax.shard_map(
        per_device,
        mesh=finer,
        in_specs=(
            P(FS, TP),
            P(),
            P(FS, TP),
            P(FS, TP),
            P(FS, TP),
            P(FS, TP),
            P(TP, FS),
            P(),
            P(FS, TP),
            P(FS, TP),
            P(None, TP),
            P(TP),
            P(TP, FS),
        ),
        out_specs=P(FS, TP),
        check_vma=False,
    )
```

```python
import jax
import jax.numpy as jnp
import numpy as np
from jax import lax
from jax.experimental import pallas as pl
from jax.experimental.pallas import tpu as pltpu
from jax.sharding import Mesh
from jax.sharding import PartitionSpec as P


HEAD_DIM = 96
HALF = HEAD_DIM // 2
NZ, NX, NY, NC = 8, 4, 4, 2
FS = ("z", "x")
TP = ("y", "c")
EPS = 1e-06
BASE = 10000.0
F32, BF16 = jnp.float32, jnp.bfloat16


def send(axis, k, a):
    n = {"z": NZ, "x": NX, "y": NY, "c": NC}[axis]
    return lax.ppermute(a, axis, [(i, (i + k) % n) for i in range(n)])


def near_z(own):
    return [send("z", k, own) for k in (-1, -2, 2, 1)]


def mixer_z(own):
    half = own.shape[0] // 2
    b1, b2, f2, f1 = near_z(own)
    f3, b3 = send("z", 1, f2), send("z", -1, b2)
    lo, hi = send("z", 2, f2[:half]), send("z", -2, b2[half:])
    return [own, b1, b2, b3, lo, hi, f3, f2, f1]


def channel_z(own):
    b1, b2, f2, f1 = near_z(own)
    f3, b3 = send("z", 1, f2), send("z", -1, b2)
    return [own, b1, b2, b3, send("z", -2, b2), f3, f2, f1]


def channel_x(own):
    half = own.shape[0] // 2
    b, f = send("x", -1, own), send("x", 1, own)
    return [own, b, send("x", 1, f[:half]), send("x", -1, b[half:]), f]


def over_x(own):
    return [own] + [send("x", k, own) for k in (-1, 2, 1)]


def of_tp(own):
    same = jnp.stack([own] + [send("y", k, own) for k in (-1, 2, 1)])
    return same, send("c", 1, same)


def to_tp(keep, other):
    both = keep.astype(F32) + send("c", 1, other).astype(F32)
    out = both.astype(BF16)
    got = [send("y", k, out[k % NY]) for k in (1, 2, -1)]
    return both[0] + sum(g.astype(F32) for g in got)


def dot(a, b, ca, cb):
    return lax.dot_general(a, b, (((ca,), (cb,)), ((), ())), preferred_element_type=F32)


def normalize(ids, same, other, gain, xn):
    y, c = ids[2], ids[3]

    def square(k, total):
        for ref in (same, other):
            v = ref[k].astype(F32)
            total = total + jnp.sum(v * v, axis=0, keepdims=True)
        return total

    total = lax.fori_loop(0, NY, square, jnp.zeros((1, xn.shape[-1]), F32))
    count = NZ * NX * xn.shape[2]
    scale = lax.rsqrt(total / count + EPS)

    def fill(k, _):
        for ref, core in ((same, c), (other, 1 - c)):
            t = lax.rem(y + k, NY) * NC + core
            v = ref[k].astype(F32) * scale
            v = v * gain[t]
            xn[t] = v.astype(BF16).reshape(xn.shape[1:])
        return 0

    lax.fori_loop(0, NY, fill, 0)


def give(ids, m, block, keep, send):
    z, x, y, c = ids[0], ids[1], ids[2], ids[3]
    t = lax.rem(z + m, NZ)
    k = lax.rem(t // NC + NY - y, NY)
    mine = lax.rem(t, NC) == c
    block = block.astype(BF16).reshape(NX, -1, block.shape[-1])

    @pl.when(mine)
    def _():
        for j in range(NX):
            keep[k, lax.rem(x + j, NX)] = block[j]

    @pl.when(jnp.logical_not(mine))
    def _():
        for j in range(NX):
            send[k, lax.rem(x + j, NX)] = block[j]


def mixer_kernel(ids, same, other, gain, decay, cos, sin, turn, *refs):
    pieces, (keep, send, xn, xr, wr) = refs[:9], refs[9:]
    z, x = ids[0], ids[1]
    normalize(ids, same, other, gain, xn)
    rows = xn.shape[2]
    span = NX * rows

    def pick(m, _):
        for j in range(NX):
            xr[pl.ds(pl.multiple_of((m * NX + j) * rows, rows), rows), :] = xn[
                lax.rem(z + m, NZ), lax.rem(x + j, NX)
            ]
        return 0

    lax.fori_loop(0, NZ, pick, 0)
    place = 0
    for ref in pieces:
        wr[place : place + ref.shape[0], :] = ref[...]
        place += ref.shape[0]
    out = dot(xr[...], wr[:, : 4 * HEAD_DIM], 0, 0).astype(BF16)
    q, k, v, g = (out[:, i * HEAD_DIM : (i + 1) * HEAD_DIM] for i in range(4))
    flip = turn[...]
    qr = (q.astype(F32) * cos[...] + dot(q, flip, 1, 0) * sin[...]).astype(BF16)
    kr = (k.astype(F32) * cos[...] + dot(k, flip, 1, 0) * sin[...]) * HEAD_DIM ** (-0.5)
    kr = kr.astype(BF16)
    scores = dot(qr, kr, 1, 1) * decay[...]
    kept = dot(scores.astype(BF16), v, 1, 0)
    normed = kept * lax.rsqrt(jnp.mean(kept * kept, axis=-1, keepdims=True) + EPS)
    gate = g.astype(F32)
    gated = (normed * (gate * jax.nn.sigmoid(gate))).astype(BF16)

    def project(m, _):
        rows_m = wr[pl.ds(pl.multiple_of(m * span, span), span), 4 * HEAD_DIM :]
        give(ids, m, dot(rows_m, gated, 1, 1), keep, send)
        return 0

    lax.fori_loop(0, NZ, project, 0)


def channel_kernel(ids, same, other, gain, taps, bias, *refs):
    pieces, (keep, send, xn, xr, acc, wu, wd) = refs[:5], refs[5:]
    z, x = ids[0], ids[1]
    normalize(ids, same, other, gain, xn)
    rows = xn.shape[2]
    width = wd.shape[-1]
    place = 0
    for ref in pieces:
        for i in range(ref.shape[0] // rows):
            j, m = divmod(place, NZ)
            wu[j, m * rows : (m + 1) * rows, :] = ref[i * rows : (i + 1) * rows, : 2 * width]
            wd[m, j * rows : (j + 1) * rows, :] = ref[i * rows : (i + 1) * rows, 2 * width :]
            place += 1
    acc[...] = jnp.zeros_like(acc)

    def expand(j, _):
        for m in range(NZ):
            xr[m * rows : (m + 1) * rows, :] = xn[lax.rem(z + m, NZ), lax.rem(x + j, NX)]
        acc[...] += dot(xr[...], wu[j], 0, 0)
        return 0

    lax.fori_loop(0, NX, expand, 0)
    gate = acc[:, :width].astype(BF16).astype(F32)
    value = acc[:, width:].astype(BF16).astype(F32)
    taps_n = taps.shape[0]
    row = lax.broadcasted_iota(jnp.int32, gate.shape, 0)
    total = jnp.zeros_like(gate) + bias[...]
    for i in range(taps_n):
        back = taps_n - 1 - i
        moved = gate if back == 0 else jnp.where(row >= back, pltpu.roll(gate, back, 0), 0.0)
        total = total + moved * taps[i : i + 1, :]
    hidden = (total * jax.nn.sigmoid(total) * value).astype(BF16)

    def project(m, _):
        give(ids, m, dot(wd[m], hidden, 1, 1), keep, send)
        return 0

    lax.fori_loop(0, NZ, project, 0)


def call(kernel, ids, args, length, rows, scratch, flops, moved):
    out = jax.ShapeDtypeStruct((NY, NX, rows, length), BF16)
    vmem = pl.BlockSpec(memory_space=pltpu.VMEM)
    run = pl.pallas_call(
        kernel,
        out_shape=(out, out),
        in_specs=[pl.BlockSpec(memory_space=pltpu.SMEM)] + [vmem] * len(args),
        out_specs=(vmem, vmem),
        scratch_shapes=scratch,
        compiler_params=pltpu.CompilerParams(vmem_limit_bytes=48 * 1024 * 1024),
        cost_estimate=pl.CostEstimate(flops=flops, bytes_accessed=moved, transcendentals=0),
    )
    keep, other = run(ids, *args)
    span = NX * rows
    return keep.reshape(NY, span, length), other.reshape(NY, span, length)


def tables(length):
    inv = np.power(np.float32(BASE), -np.arange(HALF, dtype=np.float32) / np.float32(HALF))
    angles = np.arange(length, dtype=np.float32)[:, None] * inv.astype(np.float32)[None, :]
    cos, sin = np.cos(angles).astype(np.float32), np.sin(angles).astype(np.float32)
    turn = np.zeros((HEAD_DIM, HEAD_DIM), np.float32)
    for i in range(HALF):
        turn[i + HALF, i] = -1.0
        turn[i, i + HALF] = 1.0
    return np.concatenate([cos, cos], 1), np.concatenate([sin, sin], 1), turn


def per_device(
    tokens,
    norm_in_gain,
    query_w,
    key_w,
    value_w,
    gate_w,
    out_w,
    norm_mid_gain,
    up_gate_w,
    up_value_w,
    conv_taps,
    conv_bias,
    down_w,
):
    length = tokens.shape[0]
    rows = query_w.shape[0]
    span = NX * rows
    width = conv_bias.shape[0]
    z, x, y, c = (lax.axis_index(a) for a in ("z", "x", "y", "c"))
    ids = jnp.stack([z, x, y, c]).astype(jnp.int32)
    own = tokens.T

    block = jnp.concatenate([up_gate_w, up_value_w, down_w.T], axis=1)
    channel_w = channel_x(jnp.concatenate(channel_z(block), axis=0))
    attn = jnp.concatenate([query_w, key_w, value_w, gate_w, out_w.T], axis=1)
    gains = [g.reshape(NZ, span, 1) for g in (norm_in_gain, norm_mid_gain)]
    quads, gain_in, gain_mid = lax.optimization_barrier((over_x(attn), *gains))
    mixer_w = mixer_z(jnp.concatenate(quads, axis=0))

    head = (y * NC + c).astype(F32)
    log_gamma = jnp.log1p(-jnp.exp2(-5.0 - head))
    lag = jnp.arange(length, dtype=F32)[:, None] - jnp.arange(length, dtype=F32)[None, :]
    decay = jnp.where(lag >= 0, jnp.exp(log_gamma * jnp.maximum(lag, 0.0)), 0.0)
    cos, sin, turn = tables(length)

    features = NZ * span
    canon = (NZ, NX, rows, length)
    same, other = of_tp(own)
    keep, other = call(
        mixer_kernel,
        ids,
        [same, other, gain_in, decay, jnp.asarray(cos), jnp.asarray(sin)]
        + [jnp.asarray(turn, BF16)]
        + mixer_w,
        length,
        rows,
        [
            pltpu.VMEM(canon, BF16),
            pltpu.VMEM((features, length), BF16),
            pltpu.VMEM((features, attn.shape[1]), BF16),
        ],
        2 * length * features * attn.shape[1] * 2,
        8 * features * length,
    )
    middle = (own.astype(F32) + to_tp(keep, other)).astype(BF16)
    same, other = of_tp(middle)
    keep, other = call(
        channel_kernel,
        ids,
        [same, other, gain_mid, conv_taps, conv_bias.reshape(1, width)]
        + channel_w,
        length,
        rows,
        [
            pltpu.VMEM(canon, BF16),
            pltpu.VMEM((NZ * rows, length), BF16),
            pltpu.VMEM((length, 2 * width), F32),
            pltpu.VMEM((NX, NZ * rows, 2 * width), BF16),
            pltpu.VMEM((NZ, span, width), BF16),
        ],
        2 * length * features * width * 3,
        8 * features * length,
    )
    return (middle.astype(F32) + to_tp(keep, other)).astype(BF16).T


def solution(mesh):
    finer = Mesh(mesh.devices.reshape(NZ, NX, NY, NC), ("z", "x", "y", "c"))
    return jax.shard_map(
        per_device,
        mesh=finer,
        in_specs=(
            P(FS, TP),
            P(),
            P(FS, TP),
            P(FS, TP),
            P(FS, TP),
            P(FS, TP),
            P(TP, FS),
            P(),
            P(FS, TP),
            P(FS, TP),
            P(None, TP),
            P(TP),
            P(TP, FS),
        ),
        out_specs=P(FS, TP),
        check_vma=False,
    )
```

```python
import jax
import jax.numpy as jnp
import numpy as np
from jax import lax
from jax.experimental import pallas as pl
from jax.experimental.pallas import tpu as pltpu
from jax.sharding import Mesh
from jax.sharding import PartitionSpec as P


HEAD_DIM = 96
HALF = HEAD_DIM // 2
NZ, NX, NY, NC = 8, 4, 4, 2
FS = ("z", "x")
TP = ("y", "c")
EPS = 1e-06
BASE = 10000.0
F32, BF16 = jnp.float32, jnp.bfloat16


def send(axis, k, a):
    n = {"z": NZ, "x": NX, "y": NY, "c": NC}[axis]
    return lax.ppermute(a, axis, [(i, (i + k) % n) for i in range(n)])


def mixer_z(own):
    half = own.shape[0] // 2
    b1, f1 = send("z", -1, own), send("z", 1, own)
    b2, f2 = send("z", -2, own), send("z", 2, own)
    b3 = send("z", -2, jnp.concatenate([b1, b2[:half]], axis=0))
    f3 = send("z", 2, jnp.concatenate([f2[half:], f1], axis=0))
    return [own, b1, b2, b3, f3, f2, f1]


def pairs_z(own):
    b1, f1 = send("z", -1, own), send("z", 1, own)
    far = send("z", 4, own)
    after, before = jnp.concatenate([own, b1], axis=0), jnp.concatenate([f1, own], axis=0)
    b2, f2 = send("z", -2, after), send("z", 2, before)
    return [after, b2, far, f2, f1]


def over_x(own):
    return [own] + [send("x", k, own) for k in (-1, 2, 1)]


def of_tp(own):
    same = jnp.stack([own] + [send("y", k, own) for k in (-1, 2, 1)])
    return same, send("c", 1, same)


def to_tp(keep, other):
    both = keep.astype(F32) + send("c", 1, other).astype(F32)
    out = both.astype(BF16)
    got = [send("y", k, out[k % NY]) for k in (1, 2, -1)]
    return both[0] + sum(g.astype(F32) for g in got)


def dot(a, b, ca, cb):
    return lax.dot_general(a, b, (((ca,), (cb,)), ((), ())), preferred_element_type=F32)


def normalize(ids, same, other, gain, xn):
    y, c = ids[2], ids[3]

    def square(k, total):
        for ref in (same, other):
            v = ref[k].astype(F32)
            total = total + jnp.sum(v * v, axis=0, keepdims=True)
        return total

    columns = gain[...].T
    lane = lax.broadcasted_iota(jnp.int32, columns.shape, 1)
    total = lax.fori_loop(0, NY, square, jnp.zeros((1, xn.shape[-1]), F32))
    count = NZ * NX * xn.shape[2]
    scale = lax.rsqrt(total / count + EPS)

    def fill(k, _):
        for ref, core in ((same, c), (other, 1 - c)):
            t = lax.rem(y + k, NY) * NC + core
            v = ref[k].astype(F32) * scale
            v = v * jnp.sum(jnp.where(lane == t, columns, 0.0), axis=1, keepdims=True)
            xn[t] = v.astype(BF16).reshape(xn.shape[1:])
        return 0

    lax.fori_loop(0, NY, fill, 0)


def give(ids, m, block, keep, send):
    z, x, y, c = ids[0], ids[1], ids[2], ids[3]
    t = lax.rem(z + m, NZ)
    k = lax.rem(t // NC + NY - y, NY)
    mine = lax.rem(t, NC) == c
    block = block.astype(BF16).reshape(NX, -1, block.shape[-1])

    @pl.when(mine)
    def _():
        for j in range(NX):
            keep[k, lax.rem(x + j, NX)] = block[j]

    @pl.when(jnp.logical_not(mine))
    def _():
        for j in range(NX):
            send[k, lax.rem(x + j, NX)] = block[j]


def mixer_kernel(ids, same, other, gain, log_gamma, cos, sin, turn, *refs):
    pieces, (keep, send, xn, xr, wr) = refs[:7], refs[7:]
    z, x = ids[0], ids[1]
    normalize(ids, same, other, gain, xn)
    rows = xn.shape[2]
    span = NX * rows

    def pick(m, _):
        for j in range(NX):
            xr[pl.ds(pl.multiple_of((m * NX + j) * rows, rows), rows), :] = xn[
                lax.rem(z + m, NZ), lax.rem(x + j, NX)
            ]
        return 0

    lax.fori_loop(0, NZ, pick, 0)
    place = 0
    for ref in pieces:
        wr[place : place + ref.shape[0], :] = ref[...]
        place += ref.shape[0]
    out = dot(xr[...], wr[:, : 4 * HEAD_DIM], 0, 0).astype(BF16)
    q, k, v, g = (out[:, i * HEAD_DIM : (i + 1) * HEAD_DIM] for i in range(4))
    flip = turn[...]
    qr = (q.astype(F32) * cos[...] + dot(q, flip, 1, 0) * sin[...]).astype(BF16)
    kr = (k.astype(F32) * cos[...] + dot(k, flip, 1, 0) * sin[...]) * HEAD_DIM ** (-0.5)
    kr = kr.astype(BF16)
    scores = dot(qr, kr, 1, 1)
    lag = lax.broadcasted_iota(jnp.int32, scores.shape, 0)
    lag = (lag - lax.broadcasted_iota(jnp.int32, scores.shape, 1)).astype(F32)
    decay = jnp.exp(log_gamma[...] * jnp.maximum(lag, 0.0))
    scores = jnp.where(lag >= 0, scores * decay, 0.0)
    kept = dot(scores.astype(BF16), v, 1, 0)
    normed = kept * lax.rsqrt(jnp.mean(kept * kept, axis=-1, keepdims=True) + EPS)
    gate = g.astype(F32)
    gated = (normed * (gate * jax.nn.sigmoid(gate))).astype(BF16)

    def project(m, _):
        rows_m = wr[pl.ds(pl.multiple_of(m * span, span), span), 4 * HEAD_DIM :]
        give(ids, m, dot(rows_m, gated, 1, 1), keep, send)
        return 0

    lax.fori_loop(0, NZ, project, 0)


def channel_kernel(ids, same, other, gain, taps, bias, *refs):
    ups, downs, (keep, send, xn, xr, acc, wd) = refs[:4], refs[4:9], refs[9:]
    z, x = ids[0], ids[1]
    normalize(ids, same, other, gain, xn)
    rows = xn.shape[2]
    for j in range(NX):

        def pick(m, _):
            xr[pl.ds(pl.multiple_of(m * rows, rows), rows), :] = xn[
                lax.rem(z + m, NZ), lax.rem(x + j, NX)
            ]
            return 0

        lax.fori_loop(0, NZ, pick, 0)
        part = dot(xr[...], ups[j][...], 0, 0)
        acc[...] = part if j == 0 else acc[...] + part
    width = acc.shape[1] // 2
    gate = acc[:, :width].astype(BF16).astype(F32)
    value = acc[:, width:].astype(BF16).astype(F32)
    taps_n = taps.shape[0]
    row = lax.broadcasted_iota(jnp.int32, gate.shape, 0)
    total = jnp.zeros_like(gate) + bias[...]
    for i in range(taps_n):
        back = taps_n - 1 - i
        moved = gate if back == 0 else jnp.where(row >= back, pltpu.roll(gate, back, 0), 0.0)
        total = total + moved * taps[i : i + 1, :]
    hidden = (total * jax.nn.sigmoid(total) * value).astype(BF16)

    place = 0
    for ref in downs:
        wd[place : place + ref.shape[0], :] = ref[...]
        place += ref.shape[0]
    span = NX * rows

    def project(m, _):
        rows_m = wd[pl.ds(pl.multiple_of(m * span, span), span), :]
        give(ids, m, dot(rows_m, hidden, 1, 1), keep, send)
        return 0

    lax.fori_loop(0, NZ, project, 0)


def call(kernel, ids, args, length, rows, scratch, flops, moved, grant):
    out = jax.ShapeDtypeStruct((NY, NX, rows, length), BF16)
    vmem = pl.BlockSpec(memory_space=pltpu.VMEM)
    run = pl.pallas_call(
        kernel,
        out_shape=(out, out),
        in_specs=[pl.BlockSpec(memory_space=pltpu.SMEM)] + [vmem] * len(args),
        out_specs=(vmem, vmem),
        scratch_shapes=scratch,
        compiler_params=pltpu.CompilerParams(vmem_limit_bytes=grant * 1024 * 1024),
        cost_estimate=pl.CostEstimate(flops=flops, bytes_accessed=moved, transcendentals=0),
    )
    keep, other = run(ids, *args)
    span = NX * rows
    return keep.reshape(NY, span, length), other.reshape(NY, span, length)


def tables(length):
    inv = np.power(np.float32(BASE), -np.arange(HALF, dtype=np.float32) / np.float32(HALF))
    angles = np.arange(length, dtype=np.float32)[:, None] * inv.astype(np.float32)[None, :]
    cos, sin = np.cos(angles).astype(np.float32), np.sin(angles).astype(np.float32)
    turn = np.zeros((HEAD_DIM, HEAD_DIM), np.float32)
    for i in range(HALF):
        turn[i + HALF, i] = -1.0
        turn[i, i + HALF] = 1.0
    return np.concatenate([cos, cos], 1), np.concatenate([sin, sin], 1), turn


def per_device(
    tokens,
    norm_in_gain,
    query_w,
    key_w,
    value_w,
    gate_w,
    out_w,
    norm_mid_gain,
    up_gate_w,
    up_value_w,
    conv_taps,
    conv_bias,
    down_w,
):
    length = tokens.shape[0]
    rows = query_w.shape[0]
    span = NX * rows
    width = conv_bias.shape[0]
    z, x, y, c = (lax.axis_index(a) for a in ("z", "x", "y", "c"))
    ids = jnp.stack([z, x, y, c]).astype(jnp.int32)
    own = tokens.T

    attn = jnp.concatenate([query_w, key_w, value_w, gate_w, out_w.T], axis=1)
    first = jnp.concatenate([attn, down_w.T], axis=1)
    up = jnp.concatenate([up_gate_w, up_value_w], axis=1)
    ups = over_x(jnp.concatenate(pairs_z(up), axis=0))
    quads = jnp.concatenate(over_x(first), axis=0)
    cut = attn.shape[1]
    mixer_w = mixer_z(quads[:, :cut])
    downs = pairs_z(quads[:, cut:])

    head = (y * NC + c).astype(F32)
    log_gamma = jnp.log1p(-jnp.exp2(-5.0 - head))
    cos, sin, turn = tables(length)

    features = NZ * span
    canon = (NZ, NX, rows, length)
    same, other = of_tp(own)
    keep, other = call(
        mixer_kernel,
        ids,
        [same, other, norm_in_gain.reshape(NZ, span), log_gamma.reshape(1, 1), jnp.asarray(cos)]
        + [jnp.asarray(sin)]
        + [jnp.asarray(turn, BF16)]
        + mixer_w,
        length,
        rows,
        [
            pltpu.VMEM(canon, BF16),
            pltpu.VMEM((features, length), BF16),
            pltpu.VMEM((features, cut), BF16),
        ],
        2 * length * features * cut * 2,
        8 * features * length,
        20,
    )
    middle = (own.astype(F32) + to_tp(keep, other)).astype(BF16)
    same, other = of_tp(middle)
    keep, other = call(
        channel_kernel,
        ids,
        [same, other, norm_mid_gain.reshape(NZ, span), conv_taps, conv_bias.reshape(1, width)]
        + ups
        + downs,
        length,
        rows,
        [
            pltpu.VMEM(canon, BF16),
            pltpu.VMEM((NZ * rows, length), BF16),
            pltpu.VMEM((length, 2 * width), F32),
            pltpu.VMEM((features, width), BF16),
        ],
        2 * length * features * width * 3,
        8 * features * length,
        28,
    )
    return (middle.astype(F32) + to_tp(keep, other)).astype(BF16).T


def solution(mesh):
    finer = Mesh(mesh.devices.reshape(NZ, NX, NY, NC), ("z", "x", "y", "c"))
    return jax.shard_map(
        per_device,
        mesh=finer,
        in_specs=(
            P(FS, TP),
            P(),
            P(FS, TP),
            P(FS, TP),
            P(FS, TP),
            P(FS, TP),
            P(TP, FS),
            P(),
            P(FS, TP),
            P(FS, TP),
            P(None, TP),
            P(TP),
            P(TP, FS),
        ),
        out_specs=P(FS, TP),
        check_vma=False,
    )
```

```python
import jax
import jax.numpy as jnp
import numpy as np
from jax import lax
from jax.experimental import pallas as pl
from jax.experimental.pallas import tpu as pltpu
from jax.sharding import Mesh
from jax.sharding import PartitionSpec as P


HEAD_DIM = 96
HALF = HEAD_DIM // 2
NZ, NX, NY, NC = 8, 4, 4, 2
FS = ("z", "x")
TP = ("y", "c")
EPS = 1e-06
BASE = 10000.0
F32, BF16 = jnp.float32, jnp.bfloat16


def send(axis, k, a):
    n = {"z": NZ, "x": NX, "y": NY, "c": NC}[axis]
    return lax.ppermute(a, axis, [(i, (i + k) % n) for i in range(n)])


def pairs_z(own):
    b1, f1 = send("z", -1, own), send("z", 1, own)
    far = send("z", 4, own)
    after, before = jnp.concatenate([own, b1], axis=0), jnp.concatenate([f1, own], axis=0)
    b2, f2 = send("z", -2, after), send("z", 2, before)
    return [after, b2, far, f2, f1]


def over_x(own):
    return [own] + [send("x", k, own) for k in (-1, 2, 1)]


def of_tp(own):
    same = jnp.stack([own] + [send("y", k, own) for k in (-1, 2, 1)])
    return same, send("c", 1, same)


def to_tp(keep, other):
    both = keep.astype(F32) + send("c", 1, other).astype(F32)
    out = both.astype(BF16)
    got = [send("y", k, out[k % NY]) for k in (1, 2, -1)]
    return both[0] + sum(g.astype(F32) for g in got)


def dot(a, b, ca, cb):
    return lax.dot_general(a, b, (((ca,), (cb,)), ((), ())), preferred_element_type=F32)


def normalize(ids, same, other, gain, xn):
    y, c = ids[2], ids[3]

    def square(k, total):
        for ref in (same, other):
            v = ref[k].astype(F32)
            total = total + jnp.sum(v * v, axis=0, keepdims=True)
        return total

    columns = gain[...].T
    lane = lax.broadcasted_iota(jnp.int32, columns.shape, 1)
    total = lax.fori_loop(0, NY, square, jnp.zeros((1, xn.shape[-1]), F32))
    count = NZ * NX * xn.shape[2]
    scale = lax.rsqrt(total / count + EPS)

    def fill(k, _):
        for ref, core in ((same, c), (other, 1 - c)):
            t = lax.rem(y + k, NY) * NC + core
            v = ref[k].astype(F32) * scale
            v = v * jnp.sum(jnp.where(lane == t, columns, 0.0), axis=1, keepdims=True)
            xn[t] = v.astype(BF16).reshape(xn.shape[1:])
        return 0

    lax.fori_loop(0, NY, fill, 0)


def give(ids, m, block, keep, send):
    z, x, y, c = ids[0], ids[1], ids[2], ids[3]
    t = lax.rem(z + m, NZ)
    k = lax.rem(t // NC + NY - y, NY)
    mine = lax.rem(t, NC) == c
    block = block.astype(BF16).reshape(NX, -1, block.shape[-1])

    @pl.when(mine)
    def _():
        for j in range(NX):
            keep[k, lax.rem(x + j, NX)] = block[j]

    @pl.when(jnp.logical_not(mine))
    def _():
        for j in range(NX):
            send[k, lax.rem(x + j, NX)] = block[j]


def mixer_kernel(ids, same, other, gain, log_gamma, cos, sin, turn, *refs):
    pieces, (keep, send, xn, xr, wr) = refs[:4], refs[4:]
    z, x = ids[0], ids[1]
    normalize(ids, same, other, gain, xn)
    rows = xn.shape[2]

    def pick(m, _):
        for j in range(NX):
            xr[pl.ds(pl.multiple_of((j * NZ + m) * rows, rows), rows), :] = xn[
                lax.rem(z + m, NZ), lax.rem(x + j, NX)
            ]
        return 0

    lax.fori_loop(0, NZ, pick, 0)
    place = 0
    for ref in pieces:
        wr[place : place + ref.shape[0], :] = ref[...]
        place += ref.shape[0]
    out = dot(xr[...], wr[:, : 4 * HEAD_DIM], 0, 0).astype(BF16)
    q, k, v, g = (out[:, i * HEAD_DIM : (i + 1) * HEAD_DIM] for i in range(4))
    flip = turn[...]
    qr = (q.astype(F32) * cos[...] + dot(q, flip, 1, 0) * sin[...]).astype(BF16)
    kr = (k.astype(F32) * cos[...] + dot(k, flip, 1, 0) * sin[...]) * HEAD_DIM ** (-0.5)
    kr = kr.astype(BF16)
    scores = dot(qr, kr, 1, 1)
    lag = lax.broadcasted_iota(jnp.int32, scores.shape, 0)
    lag = (lag - lax.broadcasted_iota(jnp.int32, scores.shape, 1)).astype(F32)
    decay = jnp.exp(log_gamma[...] * jnp.maximum(lag, 0.0))
    scores = jnp.where(lag >= 0, scores * decay, 0.0)
    kept = dot(scores.astype(BF16), v, 1, 0)
    normed = kept * lax.rsqrt(jnp.mean(kept * kept, axis=-1, keepdims=True) + EPS)
    gate = g.astype(F32)
    gated = (normed * (gate * jax.nn.sigmoid(gate))).astype(BF16)

    def project(m, _):
        parts = [
            wr[pl.ds(pl.multiple_of((j * NZ + m) * rows, rows), rows), 4 * HEAD_DIM :]
            for j in range(NX)
        ]
        give(ids, m, dot(jnp.concatenate(parts, axis=0), gated, 1, 1), keep, send)
        return 0

    lax.fori_loop(0, NZ, project, 0)


def channel_kernel(ids, same, other, gain, taps, bias, *refs):
    ups, downs, (keep, send, xn, xr, acc, wd) = refs[:4], refs[4:9], refs[9:]
    z, x = ids[0], ids[1]
    normalize(ids, same, other, gain, xn)
    rows = xn.shape[2]
    for j in range(NX):

        def pick(m, _):
            xr[pl.ds(pl.multiple_of(m * rows, rows), rows), :] = xn[
                lax.rem(z + m, NZ), lax.rem(x + j, NX)
            ]
            return 0

        lax.fori_loop(0, NZ, pick, 0)
        part = dot(xr[...], ups[j][...], 0, 0)
        acc[...] = part if j == 0 else acc[...] + part
    width = acc.shape[1] // 2
    gate = acc[:, :width].astype(BF16).astype(F32)
    value = acc[:, width:].astype(BF16).astype(F32)
    taps_n = taps.shape[0]
    row = lax.broadcasted_iota(jnp.int32, gate.shape, 0)
    total = jnp.zeros_like(gate) + bias[...]
    for i in range(taps_n):
        back = taps_n - 1 - i
        moved = gate if back == 0 else jnp.where(row >= back, pltpu.roll(gate, back, 0), 0.0)
        total = total + moved * taps[i : i + 1, :]
    hidden = (total * jax.nn.sigmoid(total) * value).astype(BF16)

    place = 0
    for ref in downs:
        wd[place : place + ref.shape[0], :] = ref[...]
        place += ref.shape[0]
    span = NX * rows

    def project(m, _):
        rows_m = wd[pl.ds(pl.multiple_of(m * span, span), span), :]
        give(ids, m, dot(rows_m, hidden, 1, 1), keep, send)
        return 0

    lax.fori_loop(0, NZ, project, 0)


def call(kernel, ids, args, length, rows, scratch, flops, moved, grant):
    out = jax.ShapeDtypeStruct((NY, NX, rows, length), BF16)
    vmem = pl.BlockSpec(memory_space=pltpu.VMEM)
    run = pl.pallas_call(
        kernel,
        out_shape=(out, out),
        in_specs=[pl.BlockSpec(memory_space=pltpu.SMEM)] + [vmem] * len(args),
        out_specs=(vmem, vmem),
        scratch_shapes=scratch,
        compiler_params=pltpu.CompilerParams(vmem_limit_bytes=grant * 1024 * 1024),
        cost_estimate=pl.CostEstimate(flops=flops, bytes_accessed=moved, transcendentals=0),
    )
    keep, other = run(ids, *args)
    span = NX * rows
    return keep.reshape(NY, span, length), other.reshape(NY, span, length)


def tables(length):
    inv = np.power(np.float32(BASE), -np.arange(HALF, dtype=np.float32) / np.float32(HALF))
    angles = np.arange(length, dtype=np.float32)[:, None] * inv.astype(np.float32)[None, :]
    cos, sin = np.cos(angles).astype(np.float32), np.sin(angles).astype(np.float32)
    turn = np.zeros((HEAD_DIM, HEAD_DIM), np.float32)
    for i in range(HALF):
        turn[i + HALF, i] = -1.0
        turn[i, i + HALF] = 1.0
    return np.concatenate([cos, cos], 1), np.concatenate([sin, sin], 1), turn


def per_device(
    tokens,
    norm_in_gain,
    query_w,
    key_w,
    value_w,
    gate_w,
    out_w,
    norm_mid_gain,
    up_gate_w,
    up_value_w,
    conv_taps,
    conv_bias,
    down_w,
):
    length = tokens.shape[0]
    rows = query_w.shape[0]
    span = NX * rows
    width = conv_bias.shape[0]
    z, x, y, c = (lax.axis_index(a) for a in ("z", "x", "y", "c"))
    ids = jnp.stack([z, x, y, c]).astype(jnp.int32)
    own = tokens.T

    attn = jnp.concatenate([query_w, key_w, value_w, gate_w, out_w.T], axis=1)
    mixer_w = over_x(jnp.concatenate(pairs_z(attn), axis=0))
    up = jnp.concatenate([up_gate_w, up_value_w], axis=1)
    ups = over_x(jnp.concatenate(pairs_z(up), axis=0))
    downs = pairs_z(jnp.concatenate(over_x(down_w.T), axis=0))
    cut = attn.shape[1]

    head = (y * NC + c).astype(F32)
    log_gamma = jnp.log1p(-jnp.exp2(-5.0 - head))
    cos, sin, turn = tables(length)

    features = NZ * span
    canon = (NZ, NX, rows, length)
    same, other = of_tp(own)
    keep, other = call(
        mixer_kernel,
        ids,
        [same, other, norm_in_gain.reshape(NZ, span), log_gamma.reshape(1, 1), jnp.asarray(cos)]
        + [jnp.asarray(sin)]
        + [jnp.asarray(turn, BF16)]
        + mixer_w,
        length,
        rows,
        [
            pltpu.VMEM(canon, BF16),
            pltpu.VMEM((features, length), BF16),
            pltpu.VMEM((features, cut), BF16),
        ],
        2 * length * features * cut * 2,
        8 * features * length,
        20,
    )
    middle = (own.astype(F32) + to_tp(keep, other)).astype(BF16)
    same, other = of_tp(middle)
    keep, other = call(
        channel_kernel,
        ids,
        [same, other, norm_mid_gain.reshape(NZ, span), conv_taps, conv_bias.reshape(1, width)]
        + ups
        + downs,
        length,
        rows,
        [
            pltpu.VMEM(canon, BF16),
            pltpu.VMEM((NZ * rows, length), BF16),
            pltpu.VMEM((length, 2 * width), F32),
            pltpu.VMEM((features, width), BF16),
        ],
        2 * length * features * width * 3,
        8 * features * length,
        28,
    )
    return (middle.astype(F32) + to_tp(keep, other)).astype(BF16).T


def solution(mesh):
    finer = Mesh(mesh.devices.reshape(NZ, NX, NY, NC), ("z", "x", "y", "c"))
    return jax.shard_map(
        per_device,
        mesh=finer,
        in_specs=(
            P(FS, TP),
            P(),
            P(FS, TP),
            P(FS, TP),
            P(FS, TP),
            P(FS, TP),
            P(TP, FS),
            P(),
            P(FS, TP),
            P(FS, TP),
            P(None, TP),
            P(TP),
            P(TP, FS),
        ),
        out_specs=P(FS, TP),
        check_vma=False,
    )
```

```python
import jax
import jax.numpy as jnp
import numpy as np
from jax import lax
from jax.experimental import pallas as pl
from jax.experimental.pallas import tpu as pltpu
from jax.sharding import Mesh
from jax.sharding import PartitionSpec as P


HEAD_DIM = 96
HALF = HEAD_DIM // 2
NZ, NX, NY, NC = 8, 4, 4, 2
FS = ("z", "x")
TP = ("y", "c")
EPS = 1e-06
BASE = 10000.0
F32, BF16 = jnp.float32, jnp.bfloat16


def send(axis, k, a):
    n = {"z": NZ, "x": NX, "y": NY, "c": NC}[axis]
    return lax.ppermute(a, axis, [(i, (i + k) % n) for i in range(n)])


def near_z(own):
    return [send("z", k, own) for k in (-1, -2, 2, 1)]


def mixer_z(own):
    half = own.shape[0] // 2
    b1, b2, f2, f1 = near_z(own)
    f3, b3 = send("z", 1, f2), send("z", -1, b2)
    lo, hi = send("z", 2, f2[:half]), send("z", -2, b2[half:])
    return [own, b1, b2, b3, lo, hi, f3, f2, f1]


def up_z(own):
    b1, b2, f2, f1 = near_z(own)
    f3, b3 = send("z", 1, f2), send("z", -1, b2)
    return [own, b1, b2, b3, send("z", -2, b2), f3, f2, f1]


def down_z(own):
    f, b = [own], [own]
    for _ in range(3):
        f.append(send("z", 1, f[-1]))
        b.append(send("z", -1, b[-1]))
    return [own, b[1], b[2], b[3], send("z", 1, f[3]), f[3], f[2], f[1]]


def over_x(own):
    return [own] + [send("x", k, own) for k in (-1, 2, 1)]


def of_tp(own):
    same = jnp.stack([own] + [send("y", k, own) for k in (-1, 2, 1)])
    return same, send("c", 1, same)


def to_tp(keep, other):
    both = keep.astype(F32) + send("c", 1, other).astype(F32)
    out = both.astype(BF16)
    got = [send("y", k, out[k % NY]) for k in (1, 2, -1)]
    return both[0] + sum(g.astype(F32) for g in got)


def dot(a, b, ca, cb):
    return lax.dot_general(a, b, (((ca,), (cb,)), ((), ())), preferred_element_type=F32)


def normalize(ids, same, other, gain, xn):
    y, c = ids[2], ids[3]

    def square(k, total):
        for ref in (same, other):
            v = ref[k].astype(F32)
            total = total + jnp.sum(v * v, axis=0, keepdims=True)
        return total

    columns = gain[...].T
    lane = lax.broadcasted_iota(jnp.int32, columns.shape, 1)
    total = lax.fori_loop(0, NY, square, jnp.zeros((1, xn.shape[-1]), F32))
    count = NZ * NX * xn.shape[2]
    scale = lax.rsqrt(total / count + EPS)

    def fill(k, _):
        for ref, core in ((same, c), (other, 1 - c)):
            t = lax.rem(y + k, NY) * NC + core
            v = ref[k].astype(F32) * scale
            v = v * jnp.sum(jnp.where(lane == t, columns, 0.0), axis=1, keepdims=True)
            xn[t] = v.astype(BF16).reshape(xn.shape[1:])
        return 0

    lax.fori_loop(0, NY, fill, 0)


def give(ids, m, block, keep, send):
    z, x, y, c = ids[0], ids[1], ids[2], ids[3]
    t = lax.rem(z + m, NZ)
    k = lax.rem(t // NC + NY - y, NY)
    mine = lax.rem(t, NC) == c
    block = block.astype(BF16).reshape(NX, -1, block.shape[-1])

    @pl.when(mine)
    def _():
        for j in range(NX):
            keep[k, lax.rem(x + j, NX)] = block[j]

    @pl.when(jnp.logical_not(mine))
    def _():
        for j in range(NX):
            send[k, lax.rem(x + j, NX)] = block[j]


def mixer_kernel(ids, same, other, gain, log_gamma, cos, sin, turn, *refs):
    pieces, (keep, send, xn, xr, wr) = refs[:9], refs[9:]
    z, x = ids[0], ids[1]
    normalize(ids, same, other, gain, xn)
    rows = xn.shape[2]
    span = NX * rows

    def pick(m, _):
        for j in range(NX):
            xr[pl.ds(pl.multiple_of((m * NX + j) * rows, rows), rows), :] = xn[
                lax.rem(z + m, NZ), lax.rem(x + j, NX)
            ]
        return 0

    lax.fori_loop(0, NZ, pick, 0)
    place = 0
    for ref in pieces:
        wr[place : place + ref.shape[0], :] = ref[...]
        place += ref.shape[0]
    out = dot(xr[...], wr[:, : 4 * HEAD_DIM], 0, 0).astype(BF16)
    q, k, v, g = (out[:, i * HEAD_DIM : (i + 1) * HEAD_DIM] for i in range(4))
    flip = turn[...]
    qr = (q.astype(F32) * cos[...] + dot(q, flip, 1, 0) * sin[...]).astype(BF16)
    kr = (k.astype(F32) * cos[...] + dot(k, flip, 1, 0) * sin[...]) * HEAD_DIM ** (-0.5)
    kr = kr.astype(BF16)
    scores = dot(qr, kr, 1, 1)
    lag = lax.broadcasted_iota(jnp.int32, scores.shape, 0)
    lag = (lag - lax.broadcasted_iota(jnp.int32, scores.shape, 1)).astype(F32)
    decay = jnp.exp(log_gamma[...] * jnp.maximum(lag, 0.0))
    scores = jnp.where(lag >= 0, scores * decay, 0.0)
    kept = dot(scores.astype(BF16), v, 1, 0)
    normed = kept * lax.rsqrt(jnp.mean(kept * kept, axis=-1, keepdims=True) + EPS)
    gate = g.astype(F32)
    gated = (normed * (gate * jax.nn.sigmoid(gate))).astype(BF16)

    def project(m, _):
        rows_m = wr[pl.ds(pl.multiple_of(m * span, span), span), 4 * HEAD_DIM :]
        give(ids, m, dot(rows_m, gated, 1, 1), keep, send)
        return 0

    lax.fori_loop(0, NZ, project, 0)


def channel_kernel(ids, same, other, gain, taps, bias, *refs):
    ups, downs, (keep, send, xn, xr, acc, wd) = refs[:4], refs[4:12], refs[12:]
    z, x = ids[0], ids[1]
    normalize(ids, same, other, gain, xn)
    rows = xn.shape[2]
    for j in range(NX):

        def pick(m, _):
            xr[pl.ds(pl.multiple_of(m * rows, rows), rows), :] = xn[
                lax.rem(z + m, NZ), lax.rem(x + j, NX)
            ]
            return 0

        lax.fori_loop(0, NZ, pick, 0)
        part = dot(xr[...], ups[j][...], 0, 0)
        acc[...] = part if j == 0 else acc[...] + part
    width = acc.shape[1] // 2
    gate = acc[:, :width].astype(BF16).astype(F32)
    value = acc[:, width:].astype(BF16).astype(F32)
    taps_n = taps.shape[0]
    row = lax.broadcasted_iota(jnp.int32, gate.shape, 0)
    total = jnp.zeros_like(gate) + bias[...]
    for i in range(taps_n):
        back = taps_n - 1 - i
        moved = gate if back == 0 else jnp.where(row >= back, pltpu.roll(gate, back, 0), 0.0)
        total = total + moved * taps[i : i + 1, :]
    hidden = (total * jax.nn.sigmoid(total) * value).astype(BF16)

    place = 0
    for ref in downs:
        wd[place : place + ref.shape[0], :] = ref[...]
        place += ref.shape[0]
    span = NX * rows

    def project(m, _):
        rows_m = wd[pl.ds(pl.multiple_of(m * span, span), span), :]
        give(ids, m, dot(rows_m, hidden, 1, 1), keep, send)
        return 0

    lax.fori_loop(0, NZ, project, 0)


def call(kernel, ids, args, length, rows, scratch, flops, moved, grant):
    out = jax.ShapeDtypeStruct((NY, NX, rows, length), BF16)
    vmem = pl.BlockSpec(memory_space=pltpu.VMEM)
    run = pl.pallas_call(
        kernel,
        out_shape=(out, out),
        in_specs=[pl.BlockSpec(memory_space=pltpu.SMEM)] + [vmem] * len(args),
        out_specs=(vmem, vmem),
        scratch_shapes=scratch,
        compiler_params=pltpu.CompilerParams(vmem_limit_bytes=grant * 1024 * 1024),
        cost_estimate=pl.CostEstimate(flops=flops, bytes_accessed=moved, transcendentals=0),
    )
    keep, other = run(ids, *args)
    span = NX * rows
    return keep.reshape(NY, span, length), other.reshape(NY, span, length)


def tables(length):
    inv = np.power(np.float32(BASE), -np.arange(HALF, dtype=np.float32) / np.float32(HALF))
    angles = np.arange(length, dtype=np.float32)[:, None] * inv.astype(np.float32)[None, :]
    cos, sin = np.cos(angles).astype(np.float32), np.sin(angles).astype(np.float32)
    turn = np.zeros((HEAD_DIM, HEAD_DIM), np.float32)
    for i in range(HALF):
        turn[i + HALF, i] = -1.0
        turn[i, i + HALF] = 1.0
    return np.concatenate([cos, cos], 1), np.concatenate([sin, sin], 1), turn


def per_device(
    tokens,
    norm_in_gain,
    query_w,
    key_w,
    value_w,
    gate_w,
    out_w,
    norm_mid_gain,
    up_gate_w,
    up_value_w,
    conv_taps,
    conv_bias,
    down_w,
):
    length = tokens.shape[0]
    rows = query_w.shape[0]
    span = NX * rows
    width = conv_bias.shape[0]
    z, x, y, c = (lax.axis_index(a) for a in ("z", "x", "y", "c"))
    ids = jnp.stack([z, x, y, c]).astype(jnp.int32)
    own = tokens.T

    attn = jnp.concatenate([query_w, key_w, value_w, gate_w, out_w.T], axis=1)
    first = jnp.concatenate([attn, down_w.T], axis=1)
    up = jnp.concatenate([up_gate_w, up_value_w], axis=1)
    ups = over_x(jnp.concatenate(up_z(up), axis=0))
    quads = jnp.concatenate(over_x(first), axis=0)
    cut = attn.shape[1]
    mixer_w = mixer_z(quads[:, :cut])
    downs = down_z(quads[:, cut:])

    head = (y * NC + c).astype(F32)
    log_gamma = jnp.log1p(-jnp.exp2(-5.0 - head))
    cos, sin, turn = tables(length)

    features = NZ * span
    canon = (NZ, NX, rows, length)
    same, other = of_tp(own)
    keep, other = call(
        mixer_kernel,
        ids,
        [same, other, norm_in_gain.reshape(NZ, span), log_gamma.reshape(1, 1), jnp.asarray(cos)]
        + [jnp.asarray(sin)]
        + [jnp.asarray(turn, BF16)]
        + mixer_w,
        length,
        rows,
        [
            pltpu.VMEM(canon, BF16),
            pltpu.VMEM((features, length), BF16),
            pltpu.VMEM((features, cut), BF16),
        ],
        2 * length * features * cut * 2,
        8 * features * length,
        20,
    )
    middle = (own.astype(F32) + to_tp(keep, other)).astype(BF16)
    same, other = of_tp(middle)
    keep, other = call(
        channel_kernel,
        ids,
        [same, other, norm_mid_gain.reshape(NZ, span), conv_taps, conv_bias.reshape(1, width)]
        + ups
        + downs,
        length,
        rows,
        [
            pltpu.VMEM(canon, BF16),
            pltpu.VMEM((NZ * rows, length), BF16),
            pltpu.VMEM((length, 2 * width), F32),
            pltpu.VMEM((features, width), BF16),
        ],
        2 * length * features * width * 3,
        8 * features * length,
        28,
    )
    return (middle.astype(F32) + to_tp(keep, other)).astype(BF16).T


def solution(mesh):
    finer = Mesh(mesh.devices.reshape(NZ, NX, NY, NC), ("z", "x", "y", "c"))
    return jax.shard_map(
        per_device,
        mesh=finer,
        in_specs=(
            P(FS, TP),
            P(),
            P(FS, TP),
            P(FS, TP),
            P(FS, TP),
            P(FS, TP),
            P(TP, FS),
            P(),
            P(FS, TP),
            P(FS, TP),
            P(None, TP),
            P(TP),
            P(TP, FS),
        ),
        out_specs=P(FS, TP),
        check_vma=False,
    )
```

```python
import jax
import jax.numpy as jnp
import numpy as np
from jax import lax
from jax.experimental import pallas as pl
from jax.experimental.pallas import tpu as pltpu
from jax.sharding import Mesh
from jax.sharding import PartitionSpec as P


HEAD_DIM = 96
HALF = HEAD_DIM // 2
NZ, NX, NY, NC = 8, 4, 4, 2
FS = ("z", "x")
TP = ("y", "c")
EPS = 1e-06
BASE = 10000.0
F32, BF16 = jnp.float32, jnp.bfloat16


def send(axis, k, a):
    n = {"z": NZ, "x": NX, "y": NY, "c": NC}[axis]
    return lax.ppermute(a, axis, [(i, (i + k) % n) for i in range(n)])


def near_z(own):
    return [send("z", k, own) for k in (-1, -2, 2, 1)]


def mixer_z(own):
    half = own.shape[0] // 2
    b1, b2, f2, f1 = near_z(own)
    f3, b3 = send("z", 1, f2), send("z", -1, b2)
    lo, hi = send("z", 2, f2[:half]), send("z", -2, b2[half:])
    return [own, b1, b2, b3, lo, hi, f3, f2, f1]


def up_z(own):
    b1, b2, f2, f1 = near_z(own)
    f3, b3 = send("z", 1, f2), send("z", -1, b2)
    return [own, b1, b2, b3, send("z", -2, b2), f3, f2, f1]


def down_z(own):
    f, b = [own], [own]
    for _ in range(3):
        f.append(send("z", 1, f[-1]))
        b.append(send("z", -1, b[-1]))
    return [own, b[1], b[2], b[3], send("z", 1, f[3]), f[3], f[2], f[1]]


def over_x(own):
    return [own] + [send("x", k, own) for k in (-1, 2, 1)]


def of_tp(own):
    same = jnp.stack([own] + [send("y", k, own) for k in (-1, 2, 1)])
    return same, send("c", 1, same)


def to_tp(keep, other):
    both = keep.astype(F32) + send("c", 1, other).astype(F32)
    out = both.astype(BF16)
    got = [send("y", k, out[k % NY]) for k in (1, 2, -1)]
    return both[0] + sum(g.astype(F32) for g in got)


def dot(a, b, ca, cb):
    return lax.dot_general(a, b, (((ca,), (cb,)), ((), ())), preferred_element_type=F32)


def normalize(ids, same, other, gain, first, xn):
    y, c = ids[2], ids[3]

    def square(k, total):
        for ref in (same, other):
            v = ref[k].astype(F32)
            total = total + jnp.sum(v * v, axis=0, keepdims=True)
        return total

    columns = gain[first : first + NZ, :].T
    lane = lax.broadcasted_iota(jnp.int32, columns.shape, 1)
    total = lax.fori_loop(0, NY, square, jnp.zeros((1, xn.shape[-1]), F32))
    count = NZ * NX * xn.shape[2]
    scale = lax.rsqrt(total / count + EPS)

    def fill(k, _):
        for ref, core in ((same, c), (other, 1 - c)):
            t = lax.rem(y + k, NY) * NC + core
            v = ref[k].astype(F32) * scale
            v = v * jnp.sum(jnp.where(lane == t, columns, 0.0), axis=1, keepdims=True)
            xn[t] = v.astype(BF16).reshape(xn.shape[1:])
        return 0

    lax.fori_loop(0, NY, fill, 0)


def give(ids, m, block, keep, send):
    z, x, y, c = ids[0], ids[1], ids[2], ids[3]
    t = lax.rem(z + m, NZ)
    k = lax.rem(t // NC + NY - y, NY)
    mine = lax.rem(t, NC) == c
    block = block.astype(BF16).reshape(NX, -1, block.shape[-1])

    @pl.when(mine)
    def _():
        for j in range(NX):
            keep[k, lax.rem(x + j, NX)] = block[j]

    @pl.when(jnp.logical_not(mine))
    def _():
        for j in range(NX):
            send[k, lax.rem(x + j, NX)] = block[j]


def mixer_kernel(ids, same, other, gain, log_gamma, cos, sin, turn, *refs):
    pieces, (keep, send, xn, xr, wr) = refs[:9], refs[9:]
    z, x = ids[0], ids[1]
    normalize(ids, same, other, gain, 0, xn)
    rows = xn.shape[2]
    span = NX * rows

    def pick(m, _):
        for j in range(NX):
            xr[pl.ds(pl.multiple_of((m * NX + j) * rows, rows), rows), :] = xn[
                lax.rem(z + m, NZ), lax.rem(x + j, NX)
            ]
        return 0

    lax.fori_loop(0, NZ, pick, 0)
    place = 0
    for ref in pieces:
        wr[place : place + ref.shape[0], :] = ref[...]
        place += ref.shape[0]
    out = dot(xr[...], wr[:, : 4 * HEAD_DIM], 0, 0).astype(BF16)
    q, k, v, g = (out[:, i * HEAD_DIM : (i + 1) * HEAD_DIM] for i in range(4))
    flip = turn[...]
    qr = (q.astype(F32) * cos[...] + dot(q, flip, 1, 0) * sin[...]).astype(BF16)
    kr = (k.astype(F32) * cos[...] + dot(k, flip, 1, 0) * sin[...]) * HEAD_DIM ** (-0.5)
    kr = kr.astype(BF16)
    scores = dot(qr, kr, 1, 1)
    lag = lax.broadcasted_iota(jnp.int32, scores.shape, 0)
    lag = (lag - lax.broadcasted_iota(jnp.int32, scores.shape, 1)).astype(F32)
    decay = jnp.exp(log_gamma[...] * jnp.maximum(lag, 0.0))
    scores = jnp.where(lag >= 0, scores * decay, 0.0)
    kept = dot(scores.astype(BF16), v, 1, 0)
    normed = kept * lax.rsqrt(jnp.mean(kept * kept, axis=-1, keepdims=True) + EPS)
    gate = g.astype(F32)
    gated = (normed * (gate * jax.nn.sigmoid(gate))).astype(BF16)

    def project(m, _):
        rows_m = wr[pl.ds(pl.multiple_of(m * span, span), span), 4 * HEAD_DIM :]
        give(ids, m, dot(rows_m, gated, 1, 1), keep, send)
        return 0

    lax.fori_loop(0, NZ, project, 0)


def channel_kernel(ids, same, other, gain, taps, *refs):
    ups, downs, (keep, send, xn, xr, acc, wd) = refs[:4], refs[4:12], refs[12:]
    z, x = ids[0], ids[1]
    normalize(ids, same, other, gain, NZ, xn)
    rows = xn.shape[2]
    for j in range(NX):

        def pick(m, _):
            xr[pl.ds(pl.multiple_of(m * rows, rows), rows), :] = xn[
                lax.rem(z + m, NZ), lax.rem(x + j, NX)
            ]
            return 0

        lax.fori_loop(0, NZ, pick, 0)
        part = dot(xr[...], ups[j][...], 0, 0)
        acc[...] = part if j == 0 else acc[...] + part
    width = acc.shape[1] // 2
    gate = acc[:, :width].astype(BF16).astype(F32)
    value = acc[:, width:].astype(BF16).astype(F32)
    taps_n = taps.shape[0] - 1
    row = lax.broadcasted_iota(jnp.int32, gate.shape, 0)
    total = jnp.zeros_like(gate) + taps[taps_n:, :]
    for i in range(taps_n):
        back = taps_n - 1 - i
        moved = gate if back == 0 else jnp.where(row >= back, pltpu.roll(gate, back, 0), 0.0)
        total = total + moved * taps[i : i + 1, :]
    hidden = (total * jax.nn.sigmoid(total) * value).astype(BF16)

    place = 0
    for ref in downs:
        wd[place : place + ref.shape[0], :] = ref[...]
        place += ref.shape[0]
    span = NX * rows

    def project(m, _):
        rows_m = wd[pl.ds(pl.multiple_of(m * span, span), span), :]
        give(ids, m, dot(rows_m, hidden, 1, 1), keep, send)
        return 0

    lax.fori_loop(0, NZ, project, 0)


def call(kernel, ids, args, length, rows, scratch, flops, moved, grant):
    out = jax.ShapeDtypeStruct((NY, NX, rows, length), BF16)
    vmem = pl.BlockSpec(memory_space=pltpu.VMEM)
    run = pl.pallas_call(
        kernel,
        out_shape=(out, out),
        in_specs=[pl.BlockSpec(memory_space=pltpu.SMEM)] + [vmem] * len(args),
        out_specs=(vmem, vmem),
        scratch_shapes=scratch,
        compiler_params=pltpu.CompilerParams(vmem_limit_bytes=grant * 1024 * 1024),
        cost_estimate=pl.CostEstimate(flops=flops, bytes_accessed=moved, transcendentals=0),
    )
    keep, other = run(ids, *args)
    span = NX * rows
    return keep.reshape(NY, span, length), other.reshape(NY, span, length)


def tables(length):
    inv = np.power(np.float32(BASE), -np.arange(HALF, dtype=np.float32) / np.float32(HALF))
    angles = np.arange(length, dtype=np.float32)[:, None] * inv.astype(np.float32)[None, :]
    cos, sin = np.cos(angles).astype(np.float32), np.sin(angles).astype(np.float32)
    turn = np.zeros((HEAD_DIM, HEAD_DIM), np.float32)
    for i in range(HALF):
        turn[i + HALF, i] = -1.0
        turn[i, i + HALF] = 1.0
    return np.concatenate([cos, cos], 1), np.concatenate([sin, sin], 1), turn


def per_device(
    tokens,
    norm_in_gain,
    query_w,
    key_w,
    value_w,
    gate_w,
    out_w,
    norm_mid_gain,
    up_gate_w,
    up_value_w,
    conv_taps,
    conv_bias,
    down_w,
):
    length = tokens.shape[0]
    rows = query_w.shape[0]
    span = NX * rows
    width = conv_bias.shape[0]
    z, x, y, c = (lax.axis_index(a) for a in ("z", "x", "y", "c"))
    ids = jnp.stack([z, x, y, c]).astype(jnp.int32)
    own = tokens.T

    attn = jnp.concatenate([query_w, key_w, value_w, gate_w, out_w.T], axis=1)
    first = jnp.concatenate([attn, down_w.T], axis=1)
    up = jnp.concatenate([up_gate_w, up_value_w], axis=1)
    pieces = up_z(up)
    joined = jnp.concatenate(pieces, axis=0)
    ups = over_x(joined)
    quads = jnp.concatenate(over_x(first), axis=0)
    cut = attn.shape[1]
    mixer_w = mixer_z(quads[:, :cut])
    downs = down_z(quads[:, cut:])

    head = (y * NC + c).astype(F32)
    log_gamma = jnp.log1p(-jnp.exp2(-5.0 - head))
    cos, sin, turn = tables(length)

    features = NZ * span
    gains = jnp.concatenate([norm_in_gain, norm_mid_gain]).reshape(2 * NZ, span)
    filters = jnp.concatenate([conv_taps, conv_bias[None]], axis=0)
    gains, filters = lax.optimization_barrier((gains, filters))
    canon = (NZ, NX, rows, length)
    same, other = of_tp(own)
    keep, other = call(
        mixer_kernel,
        ids,
        [same, other, gains, log_gamma.reshape(1, 1), jnp.asarray(cos)]
        + [jnp.asarray(sin)]
        + [jnp.asarray(turn, BF16)]
        + mixer_w,
        length,
        rows,
        [
            pltpu.VMEM(canon, BF16),
            pltpu.VMEM((features, length), BF16),
            pltpu.VMEM((features, cut), BF16),
        ],
        2 * length * features * cut * 2,
        8 * features * length,
        12,
    )
    middle = (own.astype(F32) + to_tp(keep, other)).astype(BF16)
    same, other = of_tp(middle)
    keep, other = call(
        channel_kernel,
        ids,
        [same, other, gains, filters]
        + ups
        + downs,
        length,
        rows,
        [
            pltpu.VMEM(canon, BF16),
            pltpu.VMEM((NZ * rows, length), BF16),
            pltpu.VMEM((length, 2 * width), F32),
            pltpu.VMEM((features, width), BF16),
        ],
        2 * length * features * width * 3,
        8 * features * length,
        16,
    )
    return (middle.astype(F32) + to_tp(keep, other)).astype(BF16).T


def solution(mesh):
    finer = Mesh(mesh.devices.reshape(NZ, NX, NY, NC), ("z", "x", "y", "c"))
    return jax.shard_map(
        per_device,
        mesh=finer,
        in_specs=(
            P(FS, TP),
            P(),
            P(FS, TP),
            P(FS, TP),
            P(FS, TP),
            P(FS, TP),
            P(TP, FS),
            P(),
            P(FS, TP),
            P(FS, TP),
            P(None, TP),
            P(TP),
            P(TP, FS),
        ),
        out_specs=P(FS, TP),
        check_vma=False,
    )
```

```python
import jax
import jax.numpy as jnp
import numpy as np
from jax import lax
from jax.experimental import pallas as pl
from jax.experimental.pallas import tpu as pltpu
from jax.sharding import Mesh
from jax.sharding import PartitionSpec as P


HEAD_DIM = 96
HALF = HEAD_DIM // 2
NZ, NX, NY, NC = 8, 4, 4, 2
FS = ("z", "x")
TP = ("y", "c")
EPS = 1e-06
BASE = 10000.0
F32, BF16 = jnp.float32, jnp.bfloat16


def send(axis, k, a):
    n = {"z": NZ, "x": NX, "y": NY, "c": NC}[axis]
    return lax.ppermute(a, axis, [(i, (i + k) % n) for i in range(n)])


def near_z(own):
    return [send("z", k, own) for k in (-1, -2, 2, 1)]


def mixer_z(own):
    half = own.shape[0] // 2
    b1, b2, f2, f1 = near_z(own)
    f3, b3 = send("z", 1, f2), send("z", -1, b2)
    lo, hi = send("z", 2, f2[:half]), send("z", -2, b2[half:])
    return [own, b1, b2, b3, lo, hi, f3, f2, f1]


def up_z(own):
    b1, b2, f2, f1 = near_z(own)
    f3, b3 = send("z", 1, f2), send("z", -1, b2)
    return [own, b1, b2, b3, send("z", -2, b2), f3, f2, f1]


def down_z(own):
    f, b = [own], [own]
    for _ in range(3):
        f.append(send("z", 1, f[-1]))
        b.append(send("z", -1, b[-1]))
    return [own, b[1], b[2], b[3], send("z", 1, f[3]), f[3], f[2], f[1]]


def over_x(own):
    return [own] + [send("x", k, own) for k in (-1, 2, 1)]


def up_x(own):
    half = own.shape[0] // 2
    b, f = send("x", -1, own), send("x", 1, own)
    return [own, b, send("x", 1, f[:half]), send("x", -1, b[half:]), f]


def of_tp(own):
    same = jnp.stack([own] + [send("y", k, own) for k in (-1, 2, 1)])
    return same, send("c", 1, same)


def to_tp(keep, other):
    both = keep.astype(F32) + send("c", 1, other).astype(F32)
    out = both.astype(BF16)
    got = [send("y", k, out[k % NY]) for k in (1, 2, -1)]
    return both[0] + sum(g.astype(F32) for g in got)


def dot(a, b, ca, cb):
    return lax.dot_general(a, b, (((ca,), (cb,)), ((), ())), preferred_element_type=F32)


def normalize(ids, same, other, gain, first, xn):
    y, c = ids[2], ids[3]

    def square(k, total):
        for ref in (same, other):
            v = ref[k].astype(F32)
            total = total + jnp.sum(v * v, axis=0, keepdims=True)
        return total

    columns = gain[first : first + NZ, :].T
    lane = lax.broadcasted_iota(jnp.int32, columns.shape, 1)
    total = lax.fori_loop(0, NY, square, jnp.zeros((1, xn.shape[-1]), F32))
    count = NZ * NX * xn.shape[2]
    scale = lax.rsqrt(total / count + EPS)

    def fill(k, _):
        for ref, core in ((same, c), (other, 1 - c)):
            t = lax.rem(y + k, NY) * NC + core
            v = ref[k].astype(F32) * scale
            v = v * jnp.sum(jnp.where(lane == t, columns, 0.0), axis=1, keepdims=True)
            xn[t] = v.astype(BF16).reshape(xn.shape[1:])
        return 0

    lax.fori_loop(0, NY, fill, 0)


def give(ids, m, block, keep, send):
    z, x, y, c = ids[0], ids[1], ids[2], ids[3]
    t = lax.rem(z + m, NZ)
    k = lax.rem(t // NC + NY - y, NY)
    mine = lax.rem(t, NC) == c
    block = block.astype(BF16).reshape(NX, -1, block.shape[-1])

    @pl.when(mine)
    def _():
        for j in range(NX):
            keep[k, lax.rem(x + j, NX)] = block[j]

    @pl.when(jnp.logical_not(mine))
    def _():
        for j in range(NX):
            send[k, lax.rem(x + j, NX)] = block[j]


def mixer_kernel(ids, same, other, gain, log_gamma, cos, sin, turn, *refs):
    pieces, (keep, send, xn, xr, wr) = refs[:9], refs[9:]
    z, x = ids[0], ids[1]
    normalize(ids, same, other, gain, 0, xn)
    rows = xn.shape[2]
    span = NX * rows

    def pick(m, _):
        for j in range(NX):
            xr[pl.ds(pl.multiple_of((m * NX + j) * rows, rows), rows), :] = xn[
                lax.rem(z + m, NZ), lax.rem(x + j, NX)
            ]
        return 0

    lax.fori_loop(0, NZ, pick, 0)
    place = 0
    for ref in pieces:
        wr[place : place + ref.shape[0], :] = ref[...]
        place += ref.shape[0]
    out = dot(xr[...], wr[:, : 4 * HEAD_DIM], 0, 0).astype(BF16)
    q, k, v, g = (out[:, i * HEAD_DIM : (i + 1) * HEAD_DIM] for i in range(4))
    flip = turn[...]
    qr = (q.astype(F32) * cos[...] + dot(q, flip, 1, 0) * sin[...]).astype(BF16)
    kr = (k.astype(F32) * cos[...] + dot(k, flip, 1, 0) * sin[...]) * HEAD_DIM ** (-0.5)
    kr = kr.astype(BF16)
    scores = dot(qr, kr, 1, 1)
    lag = lax.broadcasted_iota(jnp.int32, scores.shape, 0)
    lag = (lag - lax.broadcasted_iota(jnp.int32, scores.shape, 1)).astype(F32)
    decay = jnp.exp(log_gamma[...] * jnp.maximum(lag, 0.0))
    scores = jnp.where(lag >= 0, scores * decay, 0.0)
    kept = dot(scores.astype(BF16), v, 1, 0)
    normed = kept * lax.rsqrt(jnp.mean(kept * kept, axis=-1, keepdims=True) + EPS)
    gate = g.astype(F32)
    gated = (normed * (gate * jax.nn.sigmoid(gate))).astype(BF16)

    def project(m, _):
        rows_m = wr[pl.ds(pl.multiple_of(m * span, span), span), 4 * HEAD_DIM :]
        give(ids, m, dot(rows_m, gated, 1, 1), keep, send)
        return 0

    lax.fori_loop(0, NZ, project, 0)


def channel_kernel(ids, same, other, gain, taps, *refs):
    ups, downs, (keep, send, xn, xr, acc, wd, wu) = refs[:5], refs[5:13], refs[13:]
    z, x = ids[0], ids[1]
    normalize(ids, same, other, gain, NZ, xn)
    rows = xn.shape[2]
    half = wu.shape[0] // 2
    wu[:half, :] = ups[2][...]
    wu[half:, :] = ups[3][...]
    blocks = [ups[0], ups[1], wu, ups[4]]
    for j in range(NX):

        def pick(m, _):
            xr[pl.ds(pl.multiple_of(m * rows, rows), rows), :] = xn[
                lax.rem(z + m, NZ), lax.rem(x + j, NX)
            ]
            return 0

        lax.fori_loop(0, NZ, pick, 0)
        part = dot(xr[...], blocks[j][...], 0, 0)
        acc[...] = part if j == 0 else acc[...] + part
    width = acc.shape[1] // 2
    gate = acc[:, :width].astype(BF16).astype(F32)
    value = acc[:, width:].astype(BF16).astype(F32)
    taps_n = taps.shape[0] - 1
    row = lax.broadcasted_iota(jnp.int32, gate.shape, 0)
    total = jnp.zeros_like(gate) + taps[taps_n:, :]
    for i in range(taps_n):
        back = taps_n - 1 - i
        moved = gate if back == 0 else jnp.where(row >= back, pltpu.roll(gate, back, 0), 0.0)
        total = total + moved * taps[i : i + 1, :]
    hidden = (total * jax.nn.sigmoid(total) * value).astype(BF16)

    place = 0
    for ref in downs:
        wd[place : place + ref.shape[0], :] = ref[...]
        place += ref.shape[0]
    span = NX * rows

    def project(m, _):
        rows_m = wd[pl.ds(pl.multiple_of(m * span, span), span), :]
        give(ids, m, dot(rows_m, hidden, 1, 1), keep, send)
        return 0

    lax.fori_loop(0, NZ, project, 0)


def call(kernel, ids, args, length, rows, scratch, flops, moved, grant):
    out = jax.ShapeDtypeStruct((NY, NX, rows, length), BF16)
    vmem = pl.BlockSpec(memory_space=pltpu.VMEM)
    run = pl.pallas_call(
        kernel,
        out_shape=(out, out),
        in_specs=[pl.BlockSpec(memory_space=pltpu.SMEM)] + [vmem] * len(args),
        out_specs=(vmem, vmem),
        scratch_shapes=scratch,
        compiler_params=pltpu.CompilerParams(vmem_limit_bytes=grant * 1024 * 1024),
        cost_estimate=pl.CostEstimate(flops=flops, bytes_accessed=moved, transcendentals=0),
    )
    keep, other = run(ids, *args)
    span = NX * rows
    return keep.reshape(NY, span, length), other.reshape(NY, span, length)


def tables(length):
    inv = np.power(np.float32(BASE), -np.arange(HALF, dtype=np.float32) / np.float32(HALF))
    angles = np.arange(length, dtype=np.float32)[:, None] * inv.astype(np.float32)[None, :]
    cos, sin = np.cos(angles).astype(np.float32), np.sin(angles).astype(np.float32)
    turn = np.zeros((HEAD_DIM, HEAD_DIM), np.float32)
    for i in range(HALF):
        turn[i + HALF, i] = -1.0
        turn[i, i + HALF] = 1.0
    return np.concatenate([cos, cos], 1), np.concatenate([sin, sin], 1), turn


def per_device(
    tokens,
    norm_in_gain,
    query_w,
    key_w,
    value_w,
    gate_w,
    out_w,
    norm_mid_gain,
    up_gate_w,
    up_value_w,
    conv_taps,
    conv_bias,
    down_w,
):
    length = tokens.shape[0]
    rows = query_w.shape[0]
    span = NX * rows
    width = conv_bias.shape[0]
    z, x, y, c = (lax.axis_index(a) for a in ("z", "x", "y", "c"))
    ids = jnp.stack([z, x, y, c]).astype(jnp.int32)
    own = tokens.T

    attn = jnp.concatenate([query_w, key_w, value_w, gate_w, out_w.T], axis=1)
    first = jnp.concatenate([attn, down_w.T], axis=1)
    up = jnp.concatenate([up_gate_w, up_value_w], axis=1)
    same, other = of_tp(own)
    pieces, other = lax.optimization_barrier((up_z(up), other))
    ups = up_x(jnp.concatenate(pieces, axis=0))
    quads = jnp.concatenate(over_x(first), axis=0)
    cut = attn.shape[1]
    mixer_w = mixer_z(quads[:, :cut])
    downs = down_z(quads[:, cut:])

    head = (y * NC + c).astype(F32)
    log_gamma = jnp.log1p(-jnp.exp2(-5.0 - head))
    cos, sin, turn = tables(length)

    features = NZ * span
    gains = jnp.concatenate([norm_in_gain, norm_mid_gain]).reshape(2 * NZ, span)
    filters = jnp.concatenate([conv_taps, conv_bias[None]], axis=0)
    gains, filters = lax.optimization_barrier((gains, filters))
    canon = (NZ, NX, rows, length)
    keep, other = call(
        mixer_kernel,
        ids,
        [same, other, gains, log_gamma.reshape(1, 1), jnp.asarray(cos)]
        + [jnp.asarray(sin)]
        + [jnp.asarray(turn, BF16)]
        + mixer_w,
        length,
        rows,
        [
            pltpu.VMEM(canon, BF16),
            pltpu.VMEM((features, length), BF16),
            pltpu.VMEM((features, cut), BF16),
        ],
        2 * length * features * cut * 2,
        8 * features * length,
        12,
    )
    middle = (own.astype(F32) + to_tp(keep, other)).astype(BF16)
    same, other = of_tp(middle)
    keep, other = call(
        channel_kernel,
        ids,
        [same, other, gains, filters]
        + ups
        + downs,
        length,
        rows,
        [
            pltpu.VMEM(canon, BF16),
            pltpu.VMEM((NZ * rows, length), BF16),
            pltpu.VMEM((length, 2 * width), F32),
            pltpu.VMEM((features, width), BF16),
            pltpu.VMEM((NZ * rows, 2 * width), BF16),
        ],
        2 * length * features * width * 3,
        8 * features * length,
        16,
    )
    return (middle.astype(F32) + to_tp(keep, other)).astype(BF16).T


def solution(mesh):
    finer = Mesh(mesh.devices.reshape(NZ, NX, NY, NC), ("z", "x", "y", "c"))
    return jax.shard_map(
        per_device,
        mesh=finer,
        in_specs=(
            P(FS, TP),
            P(),
            P(FS, TP),
            P(FS, TP),
            P(FS, TP),
            P(FS, TP),
            P(TP, FS),
            P(),
            P(FS, TP),
            P(FS, TP),
            P(None, TP),
            P(TP),
            P(TP, FS),
        ),
        out_specs=P(FS, TP),
        check_vma=False,
    )
```
